256 devices in a mesh: sp: 64 (over z, x, core), tp: 4 (over y).
Axes of the slice: x: 4, y: 4, z: 8, core: 2. Of those that a mesh axis runs over, the one named last changes fastest.
Arguments:
- queries: bfloat16 [32768, 1024], P('sp', 'tp'), may hold values from -100 to 100
- keys: bfloat16 [32768, 256], P('sp', 'tp'), may hold values from -100 to 100
- values: bfloat16 [32768, 256], P('sp', 'tp'), may hold values from -6 to 6
- sink_logits: float32 [16], P('tp'), may hold values from 2 to 6
- stream: bfloat16 [32768, 2048], P(('sp', 'tp')), may hold values from -6 to 6
- out_proj: bfloat16 [1024, 2048], P('tp'), may hold values from -0.1875 to 0.1875
- norm_gain: float32 [2048], replicated, may hold values from 0.1 to 1.9
- routes: int32 [32768, 2], P(('sp', 'tp')), may hold values from 0 to 63, all different within a row; in each aligned block of 128 rows (0 to 127, 128 to 255, ...) at most 5 rows name the same one
- route_weights: float32 [32768, 2], P(('sp', 'tp')), may hold values from 0.2 to 1
- gate_proj: bfloat16 [64, 2048, 3584], P('sp', None, 'tp'), may hold values from -0.125 to 0.125
- up_proj: bfloat16 [64, 2048, 3584], P('sp', None, 'tp'), may hold values from -0.125 to 0.125
- down_proj: bfloat16 [64, 3584, 2048], P('sp', 'tp'), may hold values from -0.09375 to 0.09375
Outputs:
- layer_out: bfloat16 [32768, 2048], P(('sp', 'tp'))
The draws below stay inside these ranges and needn't reach their ends.
Inputs may be any that keep to these rules, and one draw needn't show every extreme that they name: `routes`: each row names two different experts. Among the rows of one device after the attention (aligned blocks of 128 rows) no expert is named more than 5 times.
All inputs are finite; a program needn't handle non-finite values.
Results may differ from the reference program's by a relative error of at most 0.009.
Values may be sent and summed in bfloat16 or wider, within the bound.
No kernel may reach another device: no remote copies, remote signals or barrier semaphores. Data moves between devices by JAX's collectives and lax.ppermute only.
A program may use at most 128 MiB of HBM per device.

```python
import math
import jax
import jax.numpy as jnp
import numpy as np
from jax import lax

D = 2048
HQ = 16
HK = 4
DH = 64
WINDOW = 128
FF = 3584
TOK_DEV = 128
TOKENS = 32768
EXPERTS = 64
CAP = 5
N_SP = 64
N_TP = 4


def drawn_keys(key):
    base = jax.random.normal(jax.random.fold_in(key, 17), (TOKENS, HK * DH), jnp.float32)
    return jnp.clip(base, -100.0, 100.0)


def draw_keys(key, part):
    return drawn_keys(key).astype(jnp.bfloat16)


def draw_queries(key, part):
    base = jnp.clip(jax.random.normal(jax.random.fold_in(key, 29), (TOKENS, HQ * DH), jnp.float32), -6.0, 6.0)
    return jnp.clip(base, -100.0, 100.0).astype(jnp.bfloat16)


def level_of(rng, extent, shards, least, high):
    def one(axis_at, parts):
        heights = jax.random.uniform(jax.random.fold_in(jax.random.fold_in(rng, 6), axis_at), (parts,), jnp.float32, least / len(shards), high / len(shards))
        return jnp.repeat(jnp.exp(heights), extent[axis_at] // parts).reshape((-1,) + (1,) * (len(extent) - axis_at - 1))

    factor_of = one(*shards[0])
    for cut in shards[1:]:
        factor_of = factor_of * one(*cut)
    return factor_of


def shared_out(key, own, number, rows, number_of, top, reach, slope):
    order = jax.random.permutation(key, number_of)
    crowded, common = shares(number_of, rows * top, reach, slope, True), shares(number_of, rows * top, reach, slope, False)
    places = jnp.arange(number_of)

    def named(lengths, offset_by):
        used = int((lengths > 0).sum())
        fixed = max(1, used // 4)
        passed = fixed + (places - fixed + offset_by * (used - fixed)) % max(1, number_of - fixed)
        return jnp.zeros((number_of,), jnp.int32).at[order[jnp.where(places < fixed, places, passed)]].set(jnp.asarray(lengths, jnp.int32))

    lengths = jnp.where(number % 4 == 0, named(crowded, number // 4), named(common, number - number // 4 - 1))
    mixed = jax.random.permutation(jax.random.fold_in(own, 3), number_of)
    giver, receiver = mixed[0:number_of // 2 * 2:2], mixed[1:number_of // 2 * 2:2]
    room = jnp.minimum(lengths[giver] - 1, reach - lengths[receiver]) // 2
    room = jnp.where((giver == order[0]) | (receiver == order[0]) | (lengths[receiver] == 0), 0, jnp.maximum(room, 0))
    passed = jax.random.randint(jax.random.fold_in(own, 4), (number_of // 2,), 0, 1 << 20) % (room + 1)
    lengths = lengths.at[giver].add(-passed).at[receiver].add(passed)
    labels = jnp.searchsorted(jnp.cumsum(lengths), jnp.arange(rows * top), side="right").astype(jnp.int32)
    grid = labels.reshape(top, rows).T
    grid = grid[jax.random.permutation(jax.random.fold_in(own, 1), rows)]
    offset_by = jax.random.randint(jax.random.fold_in(own, 2), (rows, 1), 0, top)
    return jnp.take_along_axis(grid, (jnp.arange(top)[None, :] + offset_by) % top, axis=1)


def shares(number_of, total, bound, lean, full):
    portions = [(1 << 20) // math.isqrt(standing ** lean) + 1 for standing in range(1, number_of + 1)]
    largest = bound if full else min(bound, max(-(-total // number_of), total * portions[0] // sum(portions)))
    least = 1 if total - largest >= number_of - 1 else 0
    given, rest = [largest] + [least] * (number_of - 1), total - largest - least * (number_of - 1)
    while rest > 0:
        movable = [i for i in range(1, number_of) if given[i] < largest] or [i for i in range(1, number_of) if given[i] < bound]
        mass, budget = sum([portions[i] for i in movable]), rest
        for i in movable:
            more = min(bound - given[i], max(1, budget * portions[i] // mass), rest)
            given[i] = given[i] + more
            rest = rest - more
    return np.array(given)


def bell_draw(rng, shape, spread, most, cuts=(), held_as=jnp.bfloat16):
    gain = level_of(rng, shape, cuts, -0.22, 0.18) if cuts else 1.0
    entries = jax.random.normal(rng, shape, jnp.float32) * spread * gain
    return jnp.minimum(jnp.maximum(entries, -most), most).astype(held_as)


def setup_inputs(seed: int = 0) -> dict:
    streams_of = jax.random.split(jax.random.key(seed), 13)
    queries = draw_queries(jax.random.fold_in(streams_of[12], 71), 0)
    keys = draw_keys(jax.random.fold_in(streams_of[12], 71), 0)
    values = bell_draw(streams_of[2], (TOKENS, HK * DH), 1.0, 6.0, ((0, 64), (1, 4)))
    sink_logits = jnp.clip(2.0 + 4.0 * jax.random.uniform(streams_of[3], (HQ,), jnp.float32) ** level_of(streams_of[3], (HQ,), ((0, 4),), -0.2, 0.2), 2.0, 6.0)
    stream = bell_draw(streams_of[4], (TOKENS, D), 1.0, 6.0, ((0, 256),))
    out_proj = bell_draw(streams_of[5], (HQ * DH, D), (HQ * DH) ** -0.5, 0.1875, ((0, 4),))
    norm_gain = jnp.clip(1.0 + 0.18 * jax.random.normal(streams_of[6], (D,), jnp.float32), 0.1, 1.9)
    routes_keys = jax.random.split(jax.random.fold_in(streams_of[7], 1), TOKENS // TOK_DEV)
    routes_turns = jax.random.permutation(jax.random.fold_in(streams_of[7], 3), TOKENS // TOK_DEV)
    routes = jax.vmap(lambda own, number: shared_out(jax.random.fold_in(streams_of[7], 2), own, number, TOK_DEV, EXPERTS, 2, CAP, 2))(routes_keys, routes_turns).reshape((TOKENS, 2))
    route_weights = jnp.clip(0.2 + 0.8 * jax.random.uniform(streams_of[8], (TOKENS, 2), jnp.float32) ** level_of(streams_of[8], (TOKENS, 2), ((0, 256),), -0.2, 0.2), 0.2, 1.0)
    gate_proj = bell_draw(streams_of[9], (EXPERTS, D, FF), D ** -0.5, 0.125, ((0, 64), (2, 4)))
    up_proj = bell_draw(streams_of[10], (EXPERTS, D, FF), D ** -0.5, 0.125, ((0, 64), (2, 4)))
    down_proj = bell_draw(streams_of[11], (EXPERTS, FF, D), FF ** -0.5, 0.09375, ((0, 64), (1, 4)))
    return {"queries": queries, "keys": keys, "values": values, "sink_logits": sink_logits, "stream": stream, "out_proj": out_proj, "norm_gain": norm_gain, "routes": routes, "route_weights": route_weights, "gate_proj": gate_proj, "up_proj": up_proj, "down_proj": down_proj}


EPSILON = 1e-06

def attention(queries, keys, values, sink_logits):
    blocks = TOKENS // WINDOW
    group = HQ // HK
    query_blocks = queries.astype(jnp.float32).reshape(blocks, WINDOW, HK, group, DH)

    def banded(source):
        shaped = source.astype(jnp.float32).reshape(blocks, WINDOW, HK, DH)
        earlier = jnp.concatenate([jnp.zeros((1, WINDOW, HK, DH), jnp.float32), shaped[:-1]], axis=0)
        return jnp.concatenate([earlier, shaped], axis=1)
    key_band = banded(keys)
    value_band = banded(values)
    scores = jnp.einsum('nqkgd,nskd->nkgqs', query_blocks, key_band) * DH ** (-0.5)
    query_pos = jnp.arange(WINDOW, dtype=jnp.int32)[:, None] + WINDOW
    key_pos = jnp.arange(2 * WINDOW, dtype=jnp.int32)[None, :]
    distance = query_pos - key_pos
    key_abs = (jnp.arange(blocks, dtype=jnp.int32) * WINDOW - WINDOW)[:, None] + jnp.arange(2 * WINDOW, dtype=jnp.int32)[None, :]
    allowed = ((distance >= 0) & (distance < WINDOW))[None] & (key_abs >= 0)[:, None, :]
    logits = jnp.where(allowed[:, None, None], scores, -jnp.inf)
    sink_part = sink_logits.astype(jnp.float32).reshape(HK, group)[None, :, :, None]
    highest = jnp.maximum(lax.optimization_barrier(jnp.max(logits, axis=-1)), sink_part)
    expo = jnp.exp(logits - highest[..., None])
    denominator = lax.optimization_barrier(jnp.sum(expo, axis=-1)) + jnp.exp(sink_part - highest)
    weights = (expo / denominator[..., None]).astype(jnp.bfloat16)
    mixed_heads = jnp.einsum('nkgqs,nskd->nqkgd', weights.astype(jnp.float32), value_band)
    return mixed_heads.reshape(TOKENS, HQ * DH).astype(jnp.bfloat16)

def reference(queries, keys, values, sink_logits, stream, out_proj, norm_gain, routes, route_weights, gate_proj, up_proj, down_proj):
    attended = attention(queries, keys, values, sink_logits)
    mixed = stream.astype(jnp.float32) + jnp.dot(attended, out_proj, preferred_element_type=jnp.float32)
    scale = lax.rsqrt(lax.optimization_barrier(jnp.mean(mixed * mixed, axis=-1, keepdims=True)) + EPSILON)
    normed = (mixed * scale * norm_gain.astype(jnp.float32)).astype(jnp.bfloat16)
    slot_count = N_SP * N_TP * CAP
    ff_slice = FF // N_TP
    positions = jnp.arange(TOKENS, dtype=jnp.int32)

    def one_expert(running, inputs):
        gate_w, up_w, down_w, expert_id = inputs
        hit = routes == expert_id
        token_weight = lax.optimization_barrier(jnp.sum(jnp.where(hit, route_weights, jnp.float32(0.0)), axis=1))
        sort_key = jnp.where(jnp.any(hit, axis=1), positions, positions + TOKENS)
        picked = jnp.argsort(sort_key)[:slot_count].astype(jnp.int32)
        rows = normed[picked]
        gate_part = jnp.dot(rows, gate_w, preferred_element_type=jnp.float32)
        up_part = jnp.dot(rows, up_w, preferred_element_type=jnp.float32)
        hidden = (jax.nn.silu(gate_part) * up_part).astype(jnp.bfloat16)
        summed = jnp.zeros((slot_count, D), jnp.float32)
        for slice_index in range(N_TP):
            partial_value = jnp.dot(hidden[:, slice_index * ff_slice:(slice_index + 1) * ff_slice], down_w[slice_index * ff_slice:(slice_index + 1) * ff_slice], preferred_element_type=jnp.float32).astype(jnp.bfloat16)
            partial_value = lax.optimization_barrier(partial_value)
            summed = summed + partial_value.astype(jnp.float32)
        expert_out = summed.astype(jnp.bfloat16).astype(jnp.float32)
        running = running.at[picked].add(token_weight[picked][:, None] * expert_out)
        return (running, None)
    start = jnp.zeros((TOKENS, D), jnp.float32)
    routed, _ = lax.scan(one_expert, start, (gate_proj, up_proj, down_proj, jnp.arange(EXPERTS, dtype=jnp.int32)))
    return (mixed + routed).astype(jnp.bfloat16)
```

```python
import functools
import jax
import jax.numpy as jnp
from jax import lax
from jax.experimental import pallas as pl
from jax.experimental.pallas import tpu as pltpu
from jax.sharding import PartitionSpec as P

DH = 64
WINDOW = 128
EPSILON = 1e-06
CHUNKS = (5,)
LIMIT = 60000 * 1024

F32 = jnp.float32
BF16 = jnp.bfloat16


def around(value, by):
    n = lax.axis_size("tp")
    return lax.ppermute(value, "tp", [(i, (i + by) % n) for i in range(n)])


def partner(value):
    n = lax.axis_size("sp")
    return lax.ppermute(value, "sp", [(i, i ^ 1) for i in range(n)])


def dot(a, b):
    return jnp.dot(a, b, preferred_element_type=F32)


def call(body, outs, scratch=(), name=None, **kw):
    return pl.pallas_call(
        body,
        out_shape=outs,
        scratch_shapes=list(scratch),
        name=name,
        compiler_params=pltpu.CompilerParams(vmem_limit_bytes=LIMIT),
        **kw,
    )


def route_body(cap, routes_ref, w_ref, pick_ref, pick0_ref, pick1_ref, wcol_ref):
    rows = routes_ref.shape[1]
    experts = pick_ref.shape[0] // cap
    ids = lax.broadcasted_iota(jnp.int32, (experts, rows), 0)
    before = (
        lax.broadcasted_iota(jnp.int32, (rows, rows), 0)
        < lax.broadcasted_iota(jnp.int32, (rows, rows), 1)
    ).astype(F32).astype(BF16)
    hit0 = (ids == routes_ref[0:1, :]).astype(F32)
    hit1 = (ids == routes_ref[1:2, :]).astype(F32)
    rank0 = dot(hit0.astype(BF16), before)
    rank1 = dot(hit1.astype(BF16), before) + jnp.sum(hit0, axis=1, keepdims=True)
    for r in range(cap):
        at0 = jnp.where(rank0 == float(r), hit0, 0.0)
        at1 = jnp.where(rank1 == float(r), hit1, 0.0)
        here = slice(r * experts, (r + 1) * experts)
        pick0_ref[here, :] = at0.astype(BF16)
        pick1_ref[here, :] = at1.astype(BF16)
        pick_ref[here, :] = (at0 + at1).astype(BF16)
    for k in range(2):
        spread = jnp.broadcast_to(w_ref[k : k + 1, :], (rows, rows))
        wcol_ref[:, k * rows : (k + 1) * rows] = spread.T


def attend_body(me_ref, first_ref, sink_ref, q_ref, k_ref, v_ref, tail_ref, *refs):
    outs, (band_k, band_v) = refs[:4], refs[4:]
    w = WINDOW
    tok = k_ref.shape[1]
    band_k[0:DH, 0:w] = tail_ref[0:DH, :]
    band_v[0:DH, 0:w] = tail_ref[DH : 2 * DH, :]
    band_k[0:DH, w:] = k_ref[...]
    band_v[0:DH, w:] = v_ref[...]
    qpos = lax.broadcasted_iota(jnp.int32, (2 * w, 2 * w), 0) % w
    kpos = lax.broadcasted_iota(jnp.int32, (2 * w, 2 * w), 1)
    near = (kpos > qpos) & (kpos <= qpos + w)
    lower = lax.broadcasted_iota(jnp.int32, (2 * w, 1), 0) < w
    zero = jnp.zeros((DH, 2 * w), BF16)
    for i in range(4):
        n = lax.rem(me_ref[0] + i, 4)
        at = pl.multiple_of(n * w, w)
        kb = band_k[0:DH, pl.ds(at, 2 * w)]
        vb = band_v[0:DH, pl.ds(at, 2 * w)]
        hidden = jnp.where((first_ref[0] == 1) & (n == 0), w, 0)
        allowed = near & (kpos >= hidden)
        qb = q_ref[pl.ds(at, w), :]
        q2 = jnp.concatenate([qb[:, 0:w], qb[:, w:]], axis=0)
        total = None
        for h in range(2):
            kz = jnp.concatenate([kb, zero] if h == 0 else [zero, kb], axis=0)
            vz = jnp.concatenate([vb, zero] if h == 0 else [zero, vb], axis=0)
            s = dot(q2, kz) * DH ** (-0.5)
            s = jnp.where(allowed, s, -jnp.inf)
            sink = jnp.where(lower, sink_ref[h], sink_ref[2 + h])
            top = jnp.maximum(jnp.max(s, axis=1, keepdims=True), sink)
            e = jnp.exp(s - top)
            den = jnp.sum(e, axis=1, keepdims=True) + jnp.exp(sink - top)
            p = (e / den).astype(BF16)
            o = lax.dot_general(p, vz, (((1,), (1,)), ((), ())), preferred_element_type=F32)
            total = o if total is None else total + o
        outs[i][...] = jnp.concatenate([total[0:w], total[w:]], axis=1).astype(BF16)


def pack_rows(stage, rows, slot, first):
    count = rows.shape[0]
    for s in range(8):
        for k in range(2):
            at = s * 256 + k * 128
            stage[2 * slot + k, pl.ds(first + s, count, stride=8), :] = rows[:, at : at + 128]


def unpack_rows(stage, slot, first, out_ref, at, count):
    for s in range(8):
        for k in range(2):
            got = stage[2 * slot + k, pl.ds(first + s, count, stride=8), :]
            lane = s * 256 + k * 128
            out_ref[at : at + count, lane : lane + 128] = got.astype(BF16)


def load_stage(stage, ref, n):
    for k in range(2 * n):
        stage[k, 0 : ref.shape[0], :] = ref[:, k * 128 : (k + 1) * 128].astype(F32)


def store_stage(out_ref, stage, n):
    for k in range(2 * n):
        out_ref[:, k * 128 : (k + 1) * 128] = stage[k].astype(BF16)


def project_body(cap, half_ref, own_ref, p_ref, m_ref, a_ref, b_ref, ps_ref, ms_ref, as_ref, bs_ref,
                 h0_ref, h1_ref, h2_ref, h3_ref, stream_ref, gain_ref, pick_ref, mixed_ref, *refs):
    outs, (stage,) = refs[: len(CHUNKS)], refs[len(CHUNKS) :]
    h0, h1, h2, h3 = h0_ref[...], h1_ref[...], h2_ref[...], h3_ref[...]
    mid = a_ref.shape[0]
    wide = own_ref.shape[1] // 2
    for mine, (p, m, a, b) in enumerate(((ps_ref, ms_ref, as_ref, bs_ref), (p_ref, m_ref, a_ref, b_ref))):
        half = half_ref[0] if mine else 1 - half_ref[0]
        here = pl.ds(pl.multiple_of(half * wide, wide), wide)
        part = dot(h0, own_ref[:, here]) + dot(h1, p[...]) + dot(h3, m[...])
        part = part + dot(h2[:, :mid], a[...]) + dot(h2[:, mid:], b[...])
        mixed_ref[:, here] = stream_ref[:, here].astype(F32) + part
    mixed = mixed_ref[...]
    scale = lax.rsqrt(jnp.mean(mixed * mixed, axis=1, keepdims=True) + EPSILON)
    normed = (mixed * scale * gain_ref[...]).astype(BF16)
    experts = pick_ref.shape[0] // cap
    slot = 0
    for c, n in enumerate(CHUNKS):
        for r in range(n):
            rows = dot(pick_ref[slot * experts : (slot + 1) * experts, :], normed)
            pack_rows(stage, rows, r, 0)
            slot += 1
        store_stage(outs[c], stage, n)


def expert_body(n, own_ref, p_ref, m_ref, a_ref, b_ref, gate_ref, up_ref, down_ref,
                own_out, pbot_out, mtop_out, plus_out, minus_out, stage, x, act):
    step = pl.program_id(0)
    steps = pl.num_programs(0)
    h = x.shape[0] // 8
    srcs = h // n

    @pl.when(step == 0)
    def _():
        row = 0
        for ref in (own_ref, p_ref, m_ref, a_ref, b_ref):
            tall = ref.shape[0]
            load_stage(stage, ref, n)
            for half in range(tall // (8 * srcs)):
                for r in range(n):
                    unpack_rows(stage, r, half * 8 * srcs, x, row, srcs)
                    row += srcs

    both = jnp.concatenate([gate_ref[0], up_ref[0]], axis=1)
    cols = gate_ref.shape[2]
    gu = dot(x[...], both)
    g, u = gu[:, :cols], gu[:, cols:]
    act[step] = (g * (1.0 / (1.0 + jnp.exp(-g))) * u).astype(BF16)

    @pl.when(step == steps - 1)
    def _():
        hid = jnp.concatenate([act[i] for i in range(act.shape[0])], axis=1)
        wide = 256
        for t in range(down_ref.shape[2] // wide):
            here = slice(t * wide, (t + 1) * wide)
            y = dot(hid, down_ref[0, :, here]).astype(BF16)
            own_out[:, here] = y[0 : 2 * h]
            minus_out[h:, here] = y[2 * h : 3 * h]
            pbot_out[:, here] = y[3 * h : 4 * h]
            mtop_out[:, here] = y[4 * h : 5 * h]
            plus_out[h:, here] = y[5 * h : 6 * h]
            plus_out[:h, here] = y[6 * h : 7 * h]
            minus_out[:h, here] = y[7 * h : 8 * h]


def gathered_body(n, own_ref, plus_ref, minus_ref, fromleft_ref, fromright_ref, out_ref, stage):
    h = fromleft_ref.shape[0]
    srcs = h // n
    top = own_ref[:h].astype(F32) + minus_ref[h:].astype(F32) + fromleft_ref[...].astype(F32)
    bottom = own_ref[h:].astype(F32) + plus_ref[h:].astype(F32) + fromright_ref[...].astype(F32)
    for half, rows in enumerate((top, bottom)):
        for r in range(n):
            pack_rows(stage, rows[r * srcs : (r + 1) * srcs], r, half * 8 * srcs)
    store_stage(out_ref, stage, n)


def combine_body(cap, *refs):
    rets, refs = refs[: len(CHUNKS)], refs[len(CHUNKS) :]
    pick0_ref, pick1_ref, wcol_ref, mixed_ref, out_ref, stage, back = refs
    experts = pick0_ref.shape[0] // cap
    slot = 0
    for ref, n in zip(rets, CHUNKS):
        load_stage(stage, ref, n)
        for r in range(n):
            unpack_rows(stage, r, 0, back, slot * experts, experts)
            slot += 1
    rows = mixed_ref.shape[0]
    one = (((0,), (0,)), ((), ()))
    for t in range(mixed_ref.shape[1] // 256):
        here = slice(t * 256, (t + 1) * 256)
        o0 = lax.dot_general(pick0_ref[...], back[:, here], one, preferred_element_type=F32)
        o1 = lax.dot_general(pick1_ref[...], back[:, here], one, preferred_element_type=F32)
        for lane in range(0, 256, rows):
            at = slice(t * 256 + lane, t * 256 + lane + rows)
            out_ref[:, at] = (
                mixed_ref[:, at]
                + wcol_ref[:, :rows] * o0[:, lane : lane + rows]
                + wcol_ref[:, rows:] * o1[:, lane : lane + rows]
            ).astype(BF16)


def spread_rows(mine):
    half = mine.shape[0] // 2
    left, right = around(mine, 1), around(mine, -1)
    return left, right, around(left[:half], 1), around(right[half:], -1)


def on_device(queries, keys, values, sink_logits, stream, out_proj, norm_gain, routes, route_weights,
              gate_proj, up_proj, down_proj):
    vmem = pl.BlockSpec(memory_space=pltpu.VMEM)
    smem = pl.BlockSpec(memory_space=pltpu.SMEM)
    tok_sp, width = queries.shape
    rows, d = stream.shape
    experts = lax.axis_size("sp")
    cap = max(2, (5 * rows + 2 * experts - 1) // (2 * experts))
    sp, tp = lax.axis_index("sp"), lax.axis_index("tp")
    key_t, value_t = keys.T, values.T

    tail = jnp.concatenate([key_t[:, tok_sp - WINDOW :], value_t[:, tok_sp - WINDOW :]], axis=0)
    tail = lax.ppermute(tail, "sp", [(i, i + 1) for i in range(experts - 1)])

    core = lax.rem(sp, 2)
    wide = d // 2
    w_own = lax.dynamic_slice(out_proj, (0, core * wide), (width, wide))
    w_p, w_m = around(w_own, 1), around(w_own, -1)
    w_a, w_b = around(w_p[: width // 2], 1), around(w_m[width // 2 :], -1)
    w_ps, w_ms, w_as, w_bs = partner(w_p), partner(w_m), partner(w_a), partner(w_b)

    slots = experts * cap
    pick, pick0, pick1, wcol = call(
        functools.partial(route_body, cap),
        [jax.ShapeDtypeStruct((slots, rows), BF16)] * 3 + [jax.ShapeDtypeStruct((rows, 2 * rows), F32)],
        name="route",
    )(routes.T, route_weights.T)

    heads = call(
        attend_body,
        [jax.ShapeDtypeStruct((WINDOW, width), BF16)] * 4,
        [pltpu.VMEM((DH, tok_sp + WINDOW), BF16)] * 2,
        in_specs=[smem, smem, smem, vmem, vmem, vmem, vmem],
        name="attend",
    )(tp.reshape(1), (sp == 0).astype(jnp.int32).reshape(1), sink_logits, queries, key_t, value_t, tail)
    heads = [heads[0]] + [around(heads[i], i) for i in (1, 2, 3)]

    mixed, *outgoing = call(
        functools.partial(project_body, cap),
        [jax.ShapeDtypeStruct((rows, d), F32)]
        + [jax.ShapeDtypeStruct((experts * 8, 256 * n), BF16) for n in CHUNKS],
        [pltpu.VMEM((2 * max(CHUNKS), experts * 8, 128), F32)],
        in_specs=[smem] + [vmem] * 16,
        name="project",
    )(core.reshape(1), out_proj, w_p, w_m, w_a, w_b, w_ps, w_ms, w_as, w_bs, *heads, stream,
      norm_gain.reshape(1, d), pick)

    returned = []
    for c, n in enumerate(CHUNKS):
        block = outgoing[c].reshape(experts, 8, 256 * n)
        arrived = lax.all_to_all(block, "sp", 0, 0, tiled=True).reshape(experts * 8, 256 * n)
        left, right, far_a, far_b = spread_rows(arrived)
        h = experts * n // 2
        cols = 128
        hidden = gate_proj.shape[2]
        full = lambda a: pl.BlockSpec(a.shape, lambda i: (0,) * a.ndim)
        own, pbot, mtop, plus, minus = call(
            functools.partial(expert_body, n),
            [jax.ShapeDtypeStruct((k * h, d), BF16) for k in (2, 1, 1, 2, 2)],
            [
                pltpu.VMEM((2 * n, experts * 8, 128), F32),
                pltpu.VMEM((8 * h, d), BF16),
                pltpu.VMEM((hidden // cols, 8 * h, cols), BF16),
            ],
            grid=(hidden // cols,),
            in_specs=[full(v) for v in (arrived, left, right, far_a, far_b)]
            + [
                pl.BlockSpec((1, d, cols), lambda i: (0, 0, i)),
                pl.BlockSpec((1, d, cols), lambda i: (0, 0, i)),
                full(down_proj),
            ],
            out_specs=[pl.BlockSpec((k * h, d), lambda i: (0, 0)) for k in (2, 1, 1, 2, 2)],
            name="experts",
        )(arrived, left, right, far_a, far_b, gate_proj, up_proj, down_proj)
        plus, minus = around(plus, 1), around(minus, -1)
        add = lambda a, b: (a.astype(F32) + b.astype(F32)).astype(BF16)
        from_left = around(add(mtop, plus[:h]), 1)
        from_right = around(add(pbot, minus[:h]), -1)
        back = call(
            functools.partial(gathered_body, n),
            jax.ShapeDtypeStruct((experts * 8, 256 * n), BF16),
            [pltpu.VMEM((2 * n, experts * 8, 128), F32)],
            name="gathered",
        )(own, plus, minus, from_left, from_right)
        back = lax.all_to_all(back.reshape(experts, 8, 256 * n), "sp", 0, 0, tiled=True)
        returned.append(back.reshape(experts * 8, 256 * n))

    return call(
        functools.partial(combine_body, cap),
        jax.ShapeDtypeStruct((rows, d), BF16),
        [pltpu.VMEM((2 * max(CHUNKS), experts * 8, 128), F32), pltpu.VMEM((slots, d), BF16)],
        name="combine",
    )(*returned, pick0, pick1, wcol, mixed)


def solution(mesh):
    return jax.shard_map(
        on_device,
        mesh=mesh,
        in_specs=(
            P("sp", "tp"),
            P("sp", "tp"),
            P("sp", "tp"),
            P("tp"),
            P(("sp", "tp"), None),
            P("tp", None),
            P(),
            P(("sp", "tp"), None),
            P(("sp", "tp"), None),
            P("sp", None, "tp"),
            P("sp", None, "tp"),
            P("sp", "tp", None),
        ),
        out_specs=P(("sp", "tp"), None),
        check_vma=False,
    )
```

```python
import functools
import jax
import jax.numpy as jnp
from jax import lax
from jax.experimental import pallas as pl
from jax.experimental.pallas import tpu as pltpu
from jax.sharding import PartitionSpec as P


DH = 64
WINDOW = 128
EPSILON = 1e-06
CHUNKS = (5,)

F32 = jnp.float32
BF16 = jnp.bfloat16


def around(value, by):
    n = lax.axis_size("tp")
    return lax.ppermute(value, "tp", [(i, (i + by) % n) for i in range(n)])


def partner(value):
    n = lax.axis_size("sp")
    return lax.ppermute(value, "sp", [(i, i ^ 1) for i in range(n)])


def dot(a, b):
    return jnp.dot(a, b, preferred_element_type=F32)


def call(body, outs, scratch=(), mib=16, **kw):
    return pl.pallas_call(
        body,
        out_shape=outs,
        scratch_shapes=list(scratch),
        compiler_params=pltpu.CompilerParams(vmem_limit_bytes=mib << 20),
        **kw,
    )


def route_body(cap, routes_ref, w_ref, pick_ref, pick0_ref, pick1_ref, wcol_ref):
    rows = routes_ref.shape[1]
    experts = pick_ref.shape[0] // cap
    ids = lax.broadcasted_iota(jnp.int32, (experts, rows), 0)
    before = (
        lax.broadcasted_iota(jnp.int32, (rows, rows), 0)
        < lax.broadcasted_iota(jnp.int32, (rows, rows), 1)
    ).astype(F32).astype(BF16)
    hit0 = (ids == routes_ref[0:1, :]).astype(F32)
    hit1 = (ids == routes_ref[1:2, :]).astype(F32)
    rank0 = dot(hit0.astype(BF16), before)
    rank1 = dot(hit1.astype(BF16), before) + jnp.sum(hit0, axis=1, keepdims=True)
    for r in range(cap):
        at0 = jnp.where(rank0 == float(r), hit0, 0.0)
        at1 = jnp.where(rank1 == float(r), hit1, 0.0)
        here = slice(r * experts, (r + 1) * experts)
        pick0_ref[here, :] = at0.astype(BF16)
        pick1_ref[here, :] = at1.astype(BF16)
        pick_ref[here, :] = (at0 + at1).astype(BF16)
    for k in range(2):
        spread = jnp.broadcast_to(w_ref[k : k + 1, :], (rows, rows))
        wcol_ref[:, k * rows : (k + 1) * rows] = spread.T


def attend_body(me_ref, first_ref, sink_ref, q_ref, k_ref, v_ref, tail_ref, *refs):
    outs, (band_k, band_v) = refs[:4], refs[4:]
    w = WINDOW
    band_k[0:DH, 0:w] = tail_ref[0:DH, :]
    band_v[0:DH, 0:w] = tail_ref[DH : 2 * DH, :]
    band_k[0:DH, w:] = k_ref[...]
    band_v[0:DH, w:] = v_ref[...]
    qpos = lax.broadcasted_iota(jnp.int32, (2 * w, 2 * w), 0) % w
    kpos = lax.broadcasted_iota(jnp.int32, (2 * w, 2 * w), 1)
    near = (kpos > qpos) & (kpos <= qpos + w)
    lower = lax.broadcasted_iota(jnp.int32, (2 * w, 1), 0) < w
    zero = jnp.zeros((DH, 2 * w), BF16)
    for i in range(4):
        n = lax.rem(me_ref[0] + i, 4)
        at = pl.multiple_of(n * w, w)
        kb = band_k[0:DH, pl.ds(at, 2 * w)]
        vb = band_v[0:DH, pl.ds(at, 2 * w)]
        hidden = jnp.where((first_ref[0] == 1) & (n == 0), w, 0)
        allowed = near & (kpos >= hidden)
        qb = q_ref[pl.ds(at, w), :]
        q2 = jnp.concatenate([qb[:, 0:w], qb[:, w:]], axis=0)
        total = None
        for h in range(2):
            kz = jnp.concatenate([kb, zero] if h == 0 else [zero, kb], axis=0)
            vz = jnp.concatenate([vb, zero] if h == 0 else [zero, vb], axis=0)
            s = dot(q2, kz) * DH ** (-0.5)
            s = jnp.where(allowed, s, -jnp.inf)
            sink = jnp.where(lower, sink_ref[h], sink_ref[2 + h])
            top = jnp.maximum(jnp.max(s, axis=1, keepdims=True), sink)
            e = jnp.exp(s - top)
            den = jnp.sum(e, axis=1, keepdims=True) + jnp.exp(sink - top)
            p = (e / den).astype(BF16)
            o = lax.dot_general(p, vz, (((1,), (1,)), ((), ())), preferred_element_type=F32)
            total = o if total is None else total + o
        outs[i][...] = jnp.concatenate([total[0:w], total[w:]], axis=1).astype(BF16)


def pack_rows(stage, rows, slot, first):
    count = rows.shape[0]
    for s in range(8):
        for k in range(2):
            at = s * 256 + k * 128
            stage[2 * slot + k, pl.ds(first + s, count, stride=8), :] = rows[:, at : at + 128]


def unpack_rows(stage, slot, first, out_ref, at, count):
    for s in range(8):
        for k in range(2):
            got = stage[2 * slot + k, pl.ds(first + s, count, stride=8), :]
            lane = s * 256 + k * 128
            out_ref[at : at + count, lane : lane + 128] = got.astype(BF16)


def load_stage(stage, ref, n):
    for k in range(2 * n):
        stage[k, 0 : ref.shape[0], :] = ref[:, k * 128 : (k + 1) * 128].astype(F32)


def store_stage(out_ref, stage, n):
    for k in range(2 * n):
        out_ref[:, k * 128 : (k + 1) * 128] = stage[k].astype(BF16)


def project_body(cap, half_ref, p_ref, m_ref, a_ref, b_ref, ps_ref, ms_ref, as_ref, bs_ref,
                 h0_ref, h1_ref, h2_ref, h3_ref, own_hbm, stream_hbm, gain_hbm, pick_hbm, mixed_hbm, *refs):
    outs, (stage, own_ref, stream_ref, gain_ref, pick_ref, mixed_ref, sems) = refs[:-7], refs[-7:]
    fetched = [
        pltpu.make_async_copy(src, dst, sems.at[i])
        for i, (src, dst) in enumerate(
            ((own_hbm, own_ref), (stream_hbm, stream_ref), (gain_hbm, gain_ref), (pick_hbm, pick_ref))
        )
    ]
    for copy in fetched:
        copy.start()
    h0, h1, h2, h3 = h0_ref[...], h1_ref[...], h2_ref[...], h3_ref[...]
    mid = a_ref.shape[0]
    wide = own_ref.shape[1] // 2
    for mine, (p, m, a, b) in enumerate(((ps_ref, ms_ref, as_ref, bs_ref), (p_ref, m_ref, a_ref, b_ref))):
        half = half_ref[0] if mine else 1 - half_ref[0]
        here = pl.ds(pl.multiple_of(half * wide, wide), wide)
        part = dot(h1, p[...]) + dot(h3, m[...])
        mixed_ref[:, here] = part + dot(h2[:, :mid], a[...]) + dot(h2[:, mid:], b[...])
    for copy in fetched:
        copy.wait()
    mixed = mixed_ref[...] + dot(h0, own_ref[...]) + stream_ref[...].astype(F32)
    mixed_ref[...] = mixed
    kept = pltpu.make_async_copy(mixed_ref, mixed_hbm, sems.at[4])
    kept.start()
    scale = lax.rsqrt(jnp.mean(mixed * mixed, axis=1, keepdims=True) + EPSILON)
    normed = (mixed * scale * gain_ref[...]).astype(BF16)
    experts = pick_ref.shape[0] // cap
    slot = 0
    for c, n in enumerate(CHUNKS):
        for r in range(n):
            rows = dot(pick_ref[slot * experts : (slot + 1) * experts, :], normed)
            pack_rows(stage, rows, r, 0)
            slot += 1
        store_stage(outs[c], stage, n)
    kept.wait()


def expert_body(n, ins, *refs):
    blocks, (gate_ref, up_ref, down_ref) = refs[:ins], refs[ins : ins + 3]
    outs, (stage, x, act, gates, ups, downs, sems) = refs[ins + 3 : -7], refs[-7:]
    h = outs[0].shape[0]
    srcs = h // n
    cols = act.shape[2]

    def fetch(i):
        here = pl.ds(pl.multiple_of(i * cols, cols), cols)
        return (
            pltpu.make_async_copy(gate_ref.at[0, :, here], gates.at[i], sems.at[0, i]),
            pltpu.make_async_copy(up_ref.at[0, :, here], ups.at[i], sems.at[1, i]),
        )

    def fetch_down():
        return pltpu.make_async_copy(down_ref.at[0], downs, sems.at[2, 0])

    for i in range(act.shape[0]):
        for copy in fetch(i):
            copy.start()
    fetch_down().start()
    row = 0
    for ref in blocks:
        load_stage(stage, ref, n)
        for half in range(ref.shape[0] // (8 * srcs)):
            for r in range(n):
                unpack_rows(stage, r, half * 8 * srcs, x, row, srcs)
                row += srcs

    def hidden_tile(i, carry):
        for copy in fetch(i):
            copy.wait()
        both = jnp.concatenate([gates[i], ups[i]], axis=1)
        gu = dot(x[...], both)
        g, u = gu[:, :cols], gu[:, cols:]
        act[i] = (g * (1.0 / (1.0 + jnp.exp(-g))) * u).astype(BF16)
        return carry

    lax.fori_loop(0, act.shape[0], hidden_tile, 0)
    fetch_down().wait()
    hid = jnp.concatenate([act[i] for i in range(act.shape[0])], axis=1)
    wide = 256

    def out_tile(t, carry):
        here = pl.ds(pl.multiple_of(t * wide, wide), wide)
        y = dot(hid, downs[:, here]).astype(BF16)
        for k, out in enumerate(outs):
            out[:, here] = y[k * h : (k + 1) * h]
        return carry

    lax.fori_loop(0, downs.shape[1] // wide, out_tile, 0)


def gathered_body(n, own_top, own_bottom, plus_ref, minus_ref, fromleft_ref, fromright_ref, out_ref, stage):
    h = fromleft_ref.shape[0]
    srcs = h // n
    top = own_top[...].astype(F32) + minus_ref[...].astype(F32) + fromleft_ref[...].astype(F32)
    bottom = own_bottom[...].astype(F32) + plus_ref[...].astype(F32) + fromright_ref[...].astype(F32)
    for half, rows in enumerate((top, bottom)):
        for r in range(n):
            pack_rows(stage, rows[r * srcs : (r + 1) * srcs], r, half * 8 * srcs)
    store_stage(out_ref, stage, n)


def combine_body(cap, *refs):
    rets, refs = refs[: len(CHUNKS)], refs[len(CHUNKS) :]
    pick0_hbm, pick1_hbm, wcol_hbm, mixed_hbm, out_ref, stage, back = refs[:7]
    pick0_ref, pick1_ref, wcol_ref, mixed_ref, sems = refs[7:]
    fetched = [
        pltpu.make_async_copy(src, dst, sems.at[i])
        for i, (src, dst) in enumerate(
            ((pick0_hbm, pick0_ref), (pick1_hbm, pick1_ref), (wcol_hbm, wcol_ref), (mixed_hbm, mixed_ref))
        )
    ]
    for copy in fetched:
        copy.start()
    experts = pick0_ref.shape[0] // cap
    slot = 0
    for ref, n in zip(rets, CHUNKS):
        load_stage(stage, ref, n)
        for r in range(n):
            unpack_rows(stage, r, 0, back, slot * experts, experts)
            slot += 1
    for copy in fetched:
        copy.wait()
    rows = mixed_ref.shape[0]
    one = (((0,), (0,)), ((), ()))
    for t in range(mixed_ref.shape[1] // 256):
        here = slice(t * 256, (t + 1) * 256)
        o0 = lax.dot_general(pick0_ref[...], back[:, here], one, preferred_element_type=F32)
        o1 = lax.dot_general(pick1_ref[...], back[:, here], one, preferred_element_type=F32)
        for lane in range(0, 256, rows):
            at = slice(t * 256 + lane, t * 256 + lane + rows)
            out_ref[:, at] = (
                mixed_ref[:, at]
                + wcol_ref[:, :rows] * o0[:, lane : lane + rows]
                + wcol_ref[:, rows:] * o1[:, lane : lane + rows]
            ).astype(BF16)


def on_device(queries, keys, values, sink_logits, stream, out_proj, norm_gain, routes, route_weights,
              gate_proj, up_proj, down_proj):
    vmem = pl.BlockSpec(memory_space=pltpu.VMEM)
    smem = pl.BlockSpec(memory_space=pltpu.SMEM)
    tok_sp, width = queries.shape
    rows, d = stream.shape
    experts = lax.axis_size("sp")
    cap = max(2, (5 * rows + 2 * experts - 1) // (2 * experts))
    sp, tp = lax.axis_index("sp"), lax.axis_index("tp")
    key_t, value_t = keys.T, values.T

    tail = jnp.concatenate([key_t[:, tok_sp - WINDOW :], value_t[:, tok_sp - WINDOW :]], axis=0)
    tail = lax.ppermute(tail, "sp", [(i, i + 1) for i in range(experts - 1)])

    core = lax.rem(sp, 2)
    wide = d // 2
    w_own = lax.dynamic_slice(out_proj, (0, core * wide), (width, wide))
    w_p, w_m = around(w_own, 1), around(w_own, -1)

    slots = experts * cap
    pick, pick0, pick1, wcol = call(
        functools.partial(route_body, cap),
        [jax.ShapeDtypeStruct((slots, rows), BF16)] * 3 + [jax.ShapeDtypeStruct((rows, 2 * rows), F32)],
        mib=58,
    )(routes.T, route_weights.T)

    heads = call(
        attend_body,
        [jax.ShapeDtypeStruct((WINDOW, width), BF16)] * 4,
        [pltpu.VMEM((DH, tok_sp + WINDOW), BF16)] * 2,
        in_specs=[smem, smem, smem, vmem, vmem, vmem, vmem],
        mib=58,
    )(tp.reshape(1), (sp == 0).astype(jnp.int32).reshape(1), sink_logits, queries, key_t, value_t, tail)
    heads = [heads[0]] + [around(heads[i], i) for i in (1, 2, 3)]
    w_p, w_m, heads = lax.optimization_barrier((w_p, w_m, heads))
    w_a, w_b = around(w_p[: width // 2], 1), around(w_m[width // 2 :], -1)
    w_ps, w_ms, w_as, w_bs = partner(w_p), partner(w_m), partner(w_a), partner(w_b)

    hbm = pl.BlockSpec(memory_space=pltpu.HBM)
    mixed, *outgoing = call(
        functools.partial(project_body, cap),
        [jax.ShapeDtypeStruct((rows, d), F32)]
        + [jax.ShapeDtypeStruct((experts * 8, 256 * n), BF16) for n in CHUNKS],
        [
            pltpu.VMEM((2 * max(CHUNKS), experts * 8, 128), F32),
            pltpu.VMEM((width, d), BF16),
            pltpu.VMEM((rows, d), BF16),
            pltpu.VMEM((1, d), F32),
            pltpu.VMEM((slots, rows), BF16),
            pltpu.VMEM((rows, d), F32),
            pltpu.SemaphoreType.DMA((5,)),
        ],
        in_specs=[smem] + [vmem] * 12 + [hbm] * 4,
        out_specs=[hbm] + [vmem] * len(CHUNKS),
        mib=20,
    )(core.reshape(1), w_p, w_m, w_a, w_b, w_ps, w_ms, w_as, w_bs, *heads, out_proj, stream,
      norm_gain.reshape(1, d), pick)

    vm = lambda k: [vmem] * k
    cols = 128
    hidden = gate_proj.shape[2]
    n = CHUNKS[0]
    h = experts * n // 2
    add = lambda a, b: (a.astype(F32) + b.astype(F32)).astype(BF16)
    tie = lax.optimization_barrier

    def run_experts(*blocks):
        tall = sum(v.shape[0] for v in blocks) // 8 * n
        return call(
            functools.partial(expert_body, n, len(blocks)),
            [jax.ShapeDtypeStruct((h, d), BF16)] * (tall // h),
            [
                pltpu.VMEM((2 * n, experts * 8, 128), F32),
                pltpu.VMEM((tall, d), BF16),
                pltpu.VMEM((hidden // cols, tall, cols), BF16),
                pltpu.VMEM((hidden // cols, d, cols), BF16),
                pltpu.VMEM((hidden // cols, d, cols), BF16),
                pltpu.VMEM((hidden, d), BF16),
                pltpu.SemaphoreType.DMA((3, hidden // cols)),
            ],
            in_specs=vm(len(blocks)) + [hbm] * 3,
            out_specs=vm(tall // h),
            mib=28,
            cost_estimate=pl.CostEstimate(
                flops=6 * tall * d * hidden, transcendentals=tall * hidden, bytes_accessed=6 * d * hidden
            ),
        )(*blocks, gate_proj, up_proj, down_proj)

    block = outgoing[0].reshape(experts, 8, 256 * n)
    arrived = lax.all_to_all(block, "sp", 0, 0, tiled=True).reshape(experts * 8, 256 * n)
    left, right = around(arrived, 1), around(arrived, -1)
    own_top, own_bottom = run_experts(arrived)
    left, right, own_top = tie((left, right, own_top))
    half = experts * 4
    far_a, far_b = around(left[:half], 1), around(right[half:], -1)
    p_top, p_bottom, m_top, m_bottom = run_experts(left, right)
    plus = around(m_bottom, 1)
    minus = around(p_top, -1)
    far_a, far_b, m_top = tie((far_a, far_b, m_top))
    y_a, y_b = run_experts(far_a, far_b)
    top, bottom = add(m_top, around(y_a, 1)), add(p_bottom, around(y_b, -1))
    from_left, from_right = around(top, 1), around(bottom, -1)
    back = call(
        functools.partial(gathered_body, n),
        jax.ShapeDtypeStruct((experts * 8, 256 * n), BF16),
        [pltpu.VMEM((2 * n, experts * 8, 128), F32)],
        in_specs=vm(6),
        out_specs=vmem,
    )(own_top, own_bottom, plus, minus, from_left, from_right)
    back = lax.all_to_all(back.reshape(experts, 8, 256 * n), "sp", 0, 0, tiled=True)
    returned = [back.reshape(experts * 8, 256 * n)]

    return call(
        functools.partial(combine_body, cap),
        jax.ShapeDtypeStruct((rows, d), BF16),
        [
            pltpu.VMEM((2 * max(CHUNKS), experts * 8, 128), F32),
            pltpu.VMEM((slots, d), BF16),
            pltpu.VMEM((slots, rows), BF16),
            pltpu.VMEM((slots, rows), BF16),
            pltpu.VMEM((rows, 2 * rows), F32),
            pltpu.VMEM((rows, d), F32),
            pltpu.SemaphoreType.DMA((4,)),
        ],
        in_specs=vm(len(CHUNKS)) + [hbm] * 4,
        out_specs=vmem,
        mib=20,
    )(*returned, pick0, pick1, wcol, mixed)


def solution(mesh):
    return jax.shard_map(
        on_device,
        mesh=mesh,
        in_specs=(
            P("sp", "tp"),
            P("sp", "tp"),
            P("sp", "tp"),
            P("tp"),
            P(("sp", "tp"), None),
            P("tp", None),
            P(),
            P(("sp", "tp"), None),
            P(("sp", "tp"), None),
            P("sp", None, "tp"),
            P("sp", None, "tp"),
            P("sp", "tp", None),
        ),
        out_specs=P(("sp", "tp"), None),
        check_vma=False,
    )
```

```python
import functools
import jax
import jax.numpy as jnp
from jax import lax
from jax.experimental import pallas as pl
from jax.experimental.pallas import tpu as pltpu
from jax.sharding import PartitionSpec as P


DH = 64
WINDOW = 128
EPSILON = 1e-06
CHUNKS = (5,)

F32 = jnp.float32
BF16 = jnp.bfloat16


def around(value, by):
    n = lax.axis_size("tp")
    return lax.ppermute(value, "tp", [(i, (i + by) % n) for i in range(n)])


def partner(value):
    n = lax.axis_size("sp")
    return lax.ppermute(value, "sp", [(i, i ^ 1) for i in range(n)])


def dot(a, b):
    return jnp.dot(a, b, preferred_element_type=F32)


def call(body, outs, scratch=(), mib=16, **kw):
    return pl.pallas_call(
        body,
        out_shape=outs,
        scratch_shapes=list(scratch),
        compiler_params=pltpu.CompilerParams(vmem_limit_bytes=mib << 20),
        **kw,
    )


def fetch_all(pairs, sems):
    copies = [pltpu.make_async_copy(src, dst, sems.at[i]) for i, (src, dst) in enumerate(pairs)]
    for copy in copies:
        copy.start()
    return copies


def wait_all(copies):
    for copy in copies:
        copy.wait()


def route_body(cap, routes_hbm, w_hbm, pick_ref, pick0_ref, pick1_ref, wcol_ref, routes_ref, w_ref, sems):
    wait_all(fetch_all(((routes_hbm, routes_ref), (w_hbm, w_ref)), sems))
    rows = routes_ref.shape[1]
    experts = pick_ref.shape[0] // cap
    ids = lax.broadcasted_iota(jnp.int32, (experts, rows), 0)
    before = (
        lax.broadcasted_iota(jnp.int32, (rows, rows), 0)
        < lax.broadcasted_iota(jnp.int32, (rows, rows), 1)
    ).astype(F32).astype(BF16)
    hit0 = (ids == routes_ref[0:1, :]).astype(F32)
    hit1 = (ids == routes_ref[1:2, :]).astype(F32)
    rank0 = dot(hit0.astype(BF16), before)
    rank1 = dot(hit1.astype(BF16), before) + jnp.sum(hit0, axis=1, keepdims=True)
    for r in range(cap):
        at0 = jnp.where(rank0 == float(r), hit0, 0.0)
        at1 = jnp.where(rank1 == float(r), hit1, 0.0)
        here = slice(r * experts, (r + 1) * experts)
        pick0_ref[here, :] = at0.astype(BF16)
        pick1_ref[here, :] = at1.astype(BF16)
        pick_ref[here, :] = (at0 + at1).astype(BF16)
    for k in range(2):
        spread = jnp.broadcast_to(w_ref[k : k + 1, :], (rows, rows))
        wcol_ref[:, k * rows : (k + 1) * rows] = spread.T


def attend_body(me_ref, first_ref, sink_ref, q_hbm, k_hbm, v_hbm, tail_ref, *refs):
    outs, (band_k, band_v, q_ref, k_ref, v_ref, sems) = refs[:4], refs[4:]
    copies = fetch_all(((q_hbm, q_ref), (k_hbm, k_ref), (v_hbm, v_ref)), sems)
    w = WINDOW
    band_k[0:DH, 0:w] = tail_ref[0:DH, :]
    band_v[0:DH, 0:w] = tail_ref[DH : 2 * DH, :]
    wait_all(copies)
    band_k[0:DH, w:] = k_ref[...]
    band_v[0:DH, w:] = v_ref[...]
    qpos = lax.broadcasted_iota(jnp.int32, (2 * w, 2 * w), 0) % w
    kpos = lax.broadcasted_iota(jnp.int32, (2 * w, 2 * w), 1)
    near = (kpos > qpos) & (kpos <= qpos + w)
    lower = lax.broadcasted_iota(jnp.int32, (2 * w, 1), 0) < w
    zero = jnp.zeros((DH, 2 * w), BF16)
    for i in range(4):
        n = lax.rem(me_ref[0] + i, 4)
        at = pl.multiple_of(n * w, w)
        kb = band_k[0:DH, pl.ds(at, 2 * w)]
        vb = band_v[0:DH, pl.ds(at, 2 * w)]
        hidden = jnp.where((first_ref[0] == 1) & (n == 0), w, 0)
        allowed = near & (kpos >= hidden)
        qb = q_ref[pl.ds(at, w), :]
        q2 = jnp.concatenate([qb[:, 0:w], qb[:, w:]], axis=0)
        total = None
        for h in range(2):
            kz = jnp.concatenate([kb, zero] if h == 0 else [zero, kb], axis=0)
            vz = jnp.concatenate([vb, zero] if h == 0 else [zero, vb], axis=0)
            s = dot(q2, kz) * DH ** (-0.5)
            s = jnp.where(allowed, s, -jnp.inf)
            sink = jnp.where(lower, sink_ref[h], sink_ref[2 + h])
            top = jnp.maximum(jnp.max(s, axis=1, keepdims=True), sink)
            e = jnp.exp(s - top)
            den = jnp.sum(e, axis=1, keepdims=True) + jnp.exp(sink - top)
            p = (e / den).astype(BF16)
            o = lax.dot_general(p, vz, (((1,), (1,)), ((), ())), preferred_element_type=F32)
            total = o if total is None else total + o
        outs[i][...] = jnp.concatenate([total[0:w], total[w:]], axis=1).astype(BF16)


def pack_rows(stage, rows, slot, first):
    count = rows.shape[0]
    for s in range(8):
        for k in range(2):
            at = s * 256 + k * 128
            stage[2 * slot + k, pl.ds(first + s, count, stride=8), :] = rows[:, at : at + 128]


def unpack_rows(stage, slot, first, out_ref, at, count):
    for s in range(8):
        for k in range(2):
            got = stage[2 * slot + k, pl.ds(first + s, count, stride=8), :]
            lane = s * 256 + k * 128
            out_ref[pl.ds(at, count), lane : lane + 128] = got.astype(BF16)


def load_stage(stage, ref, n):
    for k in range(2 * n):
        stage[k, 0 : ref.shape[0], :] = ref[:, k * 128 : (k + 1) * 128].astype(F32)


def store_stage(out_ref, stage, n):
    for k in range(2 * n):
        out_ref[:, k * 128 : (k + 1) * 128] = stage[k].astype(BF16)


def project_body(cap, half_ref, *refs):
    mine, theirs, (h0_ref, h1_ref, h2_ref, h3_ref), refs = refs[:6], refs[6:12], refs[12:16], refs[16:]
    own_hbm, stream_hbm, gain_hbm, pick_hbm, mixed_hbm = refs[:5]
    outs, (stage, own_ref, stream_ref, gain_ref, pick_ref, mixed_ref, sems) = refs[5:-7], refs[-7:]
    fetched = fetch_all(
        ((own_hbm, own_ref), (stream_hbm, stream_ref), (gain_hbm, gain_ref), (pick_hbm, pick_ref)), sems
    )
    h0, h1, h2, h3 = h0_ref[...], h1_ref[...], h2_ref[...], h3_ref[...]
    mid = mine[0].shape[0]
    wide = own_ref.shape[1] // 2
    sides = [x for h in (h1, h3, h2) for x in (h[:, :mid], h[:, mid:])]
    for half, parts in ((half_ref[0], mine), (1 - half_ref[0], theirs)):
        here = pl.ds(pl.multiple_of(half * wide, wide), wide)
        part = None
        for side, w in zip(sides, parts):
            one = dot(side, w[...])
            part = one if part is None else part + one
        mixed_ref[:, here] = part
    wait_all(fetched)
    mixed = mixed_ref[...] + dot(h0, own_ref[...]) + stream_ref[...].astype(F32)
    mixed_ref[...] = mixed
    kept = pltpu.make_async_copy(mixed_ref, mixed_hbm, sems.at[4])
    kept.start()
    scale = lax.rsqrt(jnp.mean(mixed * mixed, axis=1, keepdims=True) + EPSILON)
    normed = (mixed * scale * gain_ref[...]).astype(BF16)
    experts = pick_ref.shape[0] // cap
    slot = 0
    for c, n in enumerate(CHUNKS):
        for r in range(n):
            rows = dot(pick_ref[slot * experts : (slot + 1) * experts, :], normed)
            pack_rows(stage, rows, r, 0)
            slot += 1
        store_stage(outs[c], stage, n)
    kept.wait()


def expert_body(n, ins, *refs):
    blocks, (gate_ref, up_ref, down_ref) = refs[:ins], refs[ins : ins + 3]
    outs, (stage, x, act, gates, ups, downs, sems) = refs[ins + 3 : -7], refs[-7:]
    h = outs[0].shape[0]
    srcs = h // n
    cols = act.shape[2]

    def fetch(i):
        here = pl.ds(pl.multiple_of(i * cols, cols), cols)
        return (
            pltpu.make_async_copy(gate_ref.at[0, :, here], gates.at[i], sems.at[0, i]),
            pltpu.make_async_copy(up_ref.at[0, :, here], ups.at[i], sems.at[1, i]),
        )

    def fetch_down():
        return pltpu.make_async_copy(down_ref.at[0], downs, sems.at[2, 0])

    for i in range(act.shape[0]):
        for copy in fetch(i):
            copy.start()
    fetch_down().start()
    row = 0
    for ref in blocks:
        load_stage(stage, ref, n)
        for half in range(ref.shape[0] // (8 * srcs)):
            first = row

            def one_slot(r, carry):
                unpack_rows(stage, r, half * 8 * srcs, x, pl.multiple_of(first + r * srcs, srcs), srcs)
                return carry

            lax.fori_loop(0, n, one_slot, 0)
            row += h

    def hidden_tile(i, carry):
        for copy in fetch(i):
            copy.wait()
        both = jnp.concatenate([gates[i], ups[i]], axis=1)
        gu = dot(x[...], both)
        g, u = gu[:, :cols], gu[:, cols:]
        act[i] = (g * (1.0 / (1.0 + jnp.exp(-g))) * u).astype(BF16)
        return carry

    lax.fori_loop(0, act.shape[0], hidden_tile, 0)
    fetch_down().wait()
    hid = jnp.concatenate([act[i] for i in range(act.shape[0])], axis=1)
    wide = 256

    def out_tile(t, carry):
        here = pl.ds(pl.multiple_of(t * wide, wide), wide)
        y = dot(hid, downs[:, here]).astype(BF16)
        for k, out in enumerate(outs):
            out[:, here] = y[k * h : (k + 1) * h]
        return carry

    lax.fori_loop(0, downs.shape[1] // wide, out_tile, 0)


def gathered_body(n, own_top, own_bottom, plus_ref, minus_ref, fromleft_ref, fromright_ref, out_ref, stage):
    h = fromleft_ref.shape[0]
    srcs = h // n
    top = own_top[...].astype(F32) + minus_ref[...].astype(F32) + fromleft_ref[...].astype(F32)
    bottom = own_bottom[...].astype(F32) + plus_ref[...].astype(F32) + fromright_ref[...].astype(F32)
    for half, rows in enumerate((top, bottom)):
        for r in range(n):
            pack_rows(stage, rows[r * srcs : (r + 1) * srcs], r, half * 8 * srcs)
    store_stage(out_ref, stage, n)


def combine_body(cap, *refs):
    rets, refs = refs[: len(CHUNKS)], refs[len(CHUNKS) :]
    pick0_hbm, pick1_hbm, wcol_hbm, mixed_hbm, out_ref, stage, back = refs[:7]
    pick0_ref, pick1_ref, wcol_ref, mixed_ref, sems = refs[7:]
    fetched = fetch_all(
        ((pick0_hbm, pick0_ref), (pick1_hbm, pick1_ref), (wcol_hbm, wcol_ref), (mixed_hbm, mixed_ref)), sems
    )
    experts = pick0_ref.shape[0] // cap
    slot = 0
    for ref, n in zip(rets, CHUNKS):
        load_stage(stage, ref, n)
        for r in range(n):
            unpack_rows(stage, r, 0, back, slot * experts, experts)
            slot += 1
    wait_all(fetched)
    rows = mixed_ref.shape[0]
    one = (((0,), (0,)), ((), ()))
    for t in range(mixed_ref.shape[1] // 256):
        here = slice(t * 256, (t + 1) * 256)
        o0 = lax.dot_general(pick0_ref[...], back[:, here], one, preferred_element_type=F32)
        o1 = lax.dot_general(pick1_ref[...], back[:, here], one, preferred_element_type=F32)
        for lane in range(0, 256, rows):
            at = slice(t * 256 + lane, t * 256 + lane + rows)
            out_ref[:, at] = (
                mixed_ref[:, at]
                + wcol_ref[:, :rows] * o0[:, lane : lane + rows]
                + wcol_ref[:, rows:] * o1[:, lane : lane + rows]
            ).astype(BF16)


def hop(up, down):
    up = around(up, 1)
    down = around(down, -1)
    return up, down


def on_device(queries, keys, values, sink_logits, stream, out_proj, norm_gain, routes, route_weights,
              gate_proj, up_proj, down_proj):
    vmem = pl.BlockSpec(memory_space=pltpu.VMEM)
    smem = pl.BlockSpec(memory_space=pltpu.SMEM)
    hbm = pl.BlockSpec(memory_space=pltpu.HBM)
    tok_sp, width = queries.shape
    rows, d = stream.shape
    experts = lax.axis_size("sp")
    cap = max(2, (5 * rows + 2 * experts - 1) // (2 * experts))
    sp, tp = lax.axis_index("sp"), lax.axis_index("tp")
    key_t, value_t = keys.T, values.T

    tail = jnp.concatenate([key_t[:, tok_sp - WINDOW :], value_t[:, tok_sp - WINDOW :]], axis=0)
    tail = lax.ppermute(tail, "sp", [(i, i + 1) for i in range(experts - 1)])

    core = lax.rem(sp, 2)
    wide = d // 2
    mid = width // 2
    w_top = lax.dynamic_slice(out_proj, (0, core * wide), (mid, wide))
    w_bottom = lax.dynamic_slice(out_proj, (mid, core * wide), (mid, wide))
    left_top, right_bottom = hop(w_top, w_bottom)
    left_bottom, right_top = hop(w_bottom, w_top)
    far_top, far_bottom = hop(left_top, right_bottom)
    gathered_w = [left_top, left_bottom, right_top, right_bottom, far_top, far_bottom]
    for k in range(6):
        gathered_w.append(partner(gathered_w[k]))

    slots = experts * cap
    pick, pick0, pick1, wcol = call(
        functools.partial(route_body, cap),
        [jax.ShapeDtypeStruct((slots, rows), BF16)] * 3 + [jax.ShapeDtypeStruct((rows, 2 * rows), F32)],
        [pltpu.VMEM((2, rows), jnp.int32), pltpu.VMEM((2, rows), F32), pltpu.SemaphoreType.DMA((2,))],
        in_specs=[hbm] * 2,
        out_specs=[vmem] * 4,
        mib=8,
    )(routes.T, route_weights.T)

    heads = call(
        attend_body,
        [jax.ShapeDtypeStruct((WINDOW, width), BF16)] * 4,
        [pltpu.VMEM((DH, tok_sp + WINDOW), BF16)] * 2
        + [
            pltpu.VMEM((tok_sp, width), BF16),
            pltpu.VMEM((DH, tok_sp), BF16),
            pltpu.VMEM((DH, tok_sp), BF16),
            pltpu.SemaphoreType.DMA((3,)),
        ],
        in_specs=[smem, smem, smem, hbm, hbm, hbm, vmem],
        out_specs=[vmem] * 4,
        mib=58,
    )(tp.reshape(1), (sp == 0).astype(jnp.int32).reshape(1), sink_logits, queries, key_t, value_t, tail)
    heads = list(heads)
    for i in (1, 2, 3):
        heads[i] = around(heads[i], i)

    mixed, *outgoing = call(
        functools.partial(project_body, cap),
        [jax.ShapeDtypeStruct((rows, d), F32)]
        + [jax.ShapeDtypeStruct((experts * 8, 256 * n), BF16) for n in CHUNKS],
        [
            pltpu.VMEM((2 * max(CHUNKS), experts * 8, 128), F32),
            pltpu.VMEM((width, d), BF16),
            pltpu.VMEM((rows, d), BF16),
            pltpu.VMEM((1, d), F32),
            pltpu.VMEM((slots, rows), BF16),
            pltpu.VMEM((rows, d), F32),
            pltpu.SemaphoreType.DMA((5,)),
        ],
        in_specs=[smem] + [vmem] * 16 + [hbm] * 4,
        out_specs=[hbm] + [vmem] * len(CHUNKS),
        mib=20,
    )(core.reshape(1), *gathered_w, *heads, out_proj, stream,
      norm_gain.reshape(1, d), pick)

    vm = lambda k: [vmem] * k
    cols = 128
    hidden = gate_proj.shape[2]
    n = CHUNKS[0]
    h = experts * n // 2
    add = lambda a, b: (a.astype(F32) + b.astype(F32)).astype(BF16)
    tie = lax.optimization_barrier

    def run_experts(*blocks):
        tall = sum(v.shape[0] for v in blocks) // 8 * n
        return call(
            functools.partial(expert_body, n, len(blocks)),
            [jax.ShapeDtypeStruct((h, d), BF16)] * (tall // h),
            [
                pltpu.VMEM((2 * n, experts * 8, 128), F32),
                pltpu.VMEM((tall, d), BF16),
                pltpu.VMEM((hidden // cols, tall, cols), BF16),
                pltpu.VMEM((hidden // cols, d, cols), BF16),
                pltpu.VMEM((hidden // cols, d, cols), BF16),
                pltpu.VMEM((hidden, d), BF16),
                pltpu.SemaphoreType.DMA((3, hidden // cols)),
            ],
            in_specs=vm(len(blocks)) + [hbm] * 3,
            out_specs=vm(tall // h),
            mib=28,
            cost_estimate=pl.CostEstimate(
                flops=6 * tall * d * hidden, transcendentals=tall * hidden, bytes_accessed=6 * d * hidden
            ),
        )(*blocks, gate_proj, up_proj, down_proj)

    block = outgoing[0].reshape(experts, 8, 256 * n)
    arrived = lax.all_to_all(block, "sp", 0, 0, tiled=True).reshape(experts * 8, 256 * n)
    half = experts * 4
    top, bottom = arrived[:half], arrived[half:]
    left_top, right_bottom = hop(top, bottom)
    left_bottom, right_top = hop(bottom, top)
    own_top, own_bottom = run_experts(arrived)
    left_top, right_bottom, own_top = tie((left_top, right_bottom, own_top))
    far_a, far_b = hop(left_top, right_bottom)
    p_top, p_bottom, m_top, m_bottom = run_experts(left_top, left_bottom, right_top, right_bottom)
    plus = around(m_bottom, 1)
    minus = around(p_top, -1)
    y_a, y_b = run_experts(far_a, far_b)
    top, bottom = add(m_top, around(y_a, 1)), add(p_bottom, around(y_b, -1))
    from_left, from_right = around(top, 1), around(bottom, -1)
    back = call(
        functools.partial(gathered_body, n),
        jax.ShapeDtypeStruct((experts * 8, 256 * n), BF16),
        [pltpu.VMEM((2 * n, experts * 8, 128), F32)],
        in_specs=vm(6),
        out_specs=vmem,
    )(own_top, own_bottom, plus, minus, from_left, from_right)
    back = lax.all_to_all(back.reshape(experts, 8, 256 * n), "sp", 0, 0, tiled=True)
    returned = [back.reshape(experts * 8, 256 * n)]

    return call(
        functools.partial(combine_body, cap),
        jax.ShapeDtypeStruct((rows, d), BF16),
        [
            pltpu.VMEM((2 * max(CHUNKS), experts * 8, 128), F32),
            pltpu.VMEM((slots, d), BF16),
            pltpu.VMEM((slots, rows), BF16),
            pltpu.VMEM((slots, rows), BF16),
            pltpu.VMEM((rows, 2 * rows), F32),
            pltpu.VMEM((rows, d), F32),
            pltpu.SemaphoreType.DMA((4,)),
        ],
        in_specs=vm(len(CHUNKS)) + [hbm] * 4,
        out_specs=vmem,
        mib=20,
    )(*returned, pick0, pick1, wcol, mixed)


def solution(mesh):
    return jax.shard_map(
        on_device,
        mesh=mesh,
        in_specs=(
            P("sp", "tp"),
            P("sp", "tp"),
            P("sp", "tp"),
            P("tp"),
            P(("sp", "tp"), None),
            P("tp", None),
            P(),
            P(("sp", "tp"), None),
            P(("sp", "tp"), None),
            P("sp", None, "tp"),
            P("sp", None, "tp"),
            P("sp", "tp", None),
        ),
        out_specs=P(("sp", "tp"), None),
        check_vma=False,
    )
```

```python
import functools
import jax
import jax.numpy as jnp
from jax import lax
from jax.experimental import pallas as pl
from jax.experimental.pallas import tpu as pltpu
from jax.sharding import PartitionSpec as P


DH = 64
WINDOW = 128
EPSILON = 1e-06
CHUNKS = (5,)

F32 = jnp.float32
BF16 = jnp.bfloat16


EVEN, ACROSS, ODD = (1, 0, 3, 2), (2, 3, 0, 1), (3, 2, 1, 0)


def exchange(value, peers):
    return lax.ppermute(value, "tp", list(enumerate(peers)))


def partner(value):
    n = lax.axis_size("sp")
    return lax.ppermute(value, "sp", [(i, i ^ 1) for i in range(n)])


def dot(a, b):
    return jnp.dot(a, b, preferred_element_type=F32)


def call(body, outs, scratch=(), mib=16, **kw):
    return pl.pallas_call(
        body,
        out_shape=outs,
        scratch_shapes=list(scratch),
        compiler_params=pltpu.CompilerParams(vmem_limit_bytes=mib << 20),
        **kw,
    )


def fetch_all(pairs, sems):
    copies = [pltpu.make_async_copy(src, dst, sems.at[i]) for i, (src, dst) in enumerate(pairs)]
    for copy in copies:
        copy.start()
    return copies


def wait_all(copies):
    for copy in copies:
        copy.wait()


def route_body(cap, routes_hbm, w_hbm, pick_ref, pick0_ref, pick1_ref, wcol_ref, routes_ref, w_ref, sems):
    wait_all(fetch_all(((routes_hbm, routes_ref), (w_hbm, w_ref)), sems))
    rows = routes_ref.shape[1]
    experts = pick_ref.shape[0] // cap
    ids = lax.broadcasted_iota(jnp.int32, (experts, rows), 0)
    before = (
        lax.broadcasted_iota(jnp.int32, (rows, rows), 0)
        < lax.broadcasted_iota(jnp.int32, (rows, rows), 1)
    ).astype(F32).astype(BF16)
    hit0 = (ids == routes_ref[0:1, :]).astype(F32)
    hit1 = (ids == routes_ref[1:2, :]).astype(F32)
    rank0 = dot(hit0.astype(BF16), before)
    rank1 = dot(hit1.astype(BF16), before) + jnp.sum(hit0, axis=1, keepdims=True)
    for r in range(cap):
        at0 = jnp.where(rank0 == float(r), hit0, 0.0)
        at1 = jnp.where(rank1 == float(r), hit1, 0.0)
        here = slice(r * experts, (r + 1) * experts)
        pick0_ref[here, :] = at0.astype(BF16)
        pick1_ref[here, :] = at1.astype(BF16)
        pick_ref[here, :] = (at0 + at1).astype(BF16)
    for k in range(2):
        spread = jnp.broadcast_to(w_ref[k : k + 1, :], (rows, rows))
        wcol_ref[:, k * rows : (k + 1) * rows] = spread.T


def split_body(half_ref, w_hbm, k_hbm, v_hbm, top_ref, bottom_ref, tail_ref, sems):
    mid, wide = top_ref.shape
    cols = pl.ds(pl.multiple_of(half_ref[0] * wide, wide), wide)
    last = pl.ds(k_hbm.shape[1] - WINDOW, WINDOW)
    copies = fetch_all(
        (
            (w_hbm.at[0:mid, cols], top_ref),
            (w_hbm.at[mid : 2 * mid, cols], bottom_ref),
            (k_hbm.at[:, last], tail_ref.at[0:DH, :]),
            (v_hbm.at[:, last], tail_ref.at[DH : 2 * DH, :]),
        ),
        sems,
    )
    wait_all(copies)


def attend_body(me_ref, first_ref, sink_ref, q_hbm, k_hbm, v_hbm, tail_ref, *refs):
    outs, (band_k, band_v, q_ref, k_ref, v_ref, sems) = refs[:4], refs[4:]
    copies = fetch_all(((q_hbm, q_ref), (k_hbm, k_ref), (v_hbm, v_ref)), sems)
    w = WINDOW
    band_k[0:DH, 0:w] = tail_ref[0:DH, :]
    band_v[0:DH, 0:w] = tail_ref[DH : 2 * DH, :]
    wait_all(copies)
    band_k[0:DH, w:] = k_ref[...]
    band_v[0:DH, w:] = v_ref[...]
    qpos = lax.broadcasted_iota(jnp.int32, (2 * w, 2 * w), 0) % w
    kpos = lax.broadcasted_iota(jnp.int32, (2 * w, 2 * w), 1)
    near = (kpos > qpos) & (kpos <= qpos + w)
    lower = lax.broadcasted_iota(jnp.int32, (2 * w, 1), 0) < w
    zero = jnp.zeros((DH, 2 * w), BF16)
    for i in range(4):
        n = me_ref[0] ^ i
        at = pl.multiple_of(n * w, w)
        kb = band_k[0:DH, pl.ds(at, 2 * w)]
        vb = band_v[0:DH, pl.ds(at, 2 * w)]
        hidden = jnp.where((first_ref[0] == 1) & (n == 0), w, 0)
        allowed = near & (kpos >= hidden)
        qb = q_ref[pl.ds(at, w), :]
        q2 = jnp.concatenate([qb[:, 0:w], qb[:, w:]], axis=0)
        total = None
        for h in range(2):
            kz = jnp.concatenate([kb, zero] if h == 0 else [zero, kb], axis=0)
            vz = jnp.concatenate([vb, zero] if h == 0 else [zero, vb], axis=0)
            s = dot(q2, kz) * DH ** (-0.5)
            s = jnp.where(allowed, s, -jnp.inf)
            sink = jnp.where(lower, sink_ref[h], sink_ref[2 + h])
            top = jnp.maximum(jnp.max(s, axis=1, keepdims=True), sink)
            e = jnp.exp(s - top)
            den = jnp.sum(e, axis=1, keepdims=True) + jnp.exp(sink - top)
            p = (e / den).astype(BF16)
            o = lax.dot_general(p, vz, (((1,), (1,)), ((), ())), preferred_element_type=F32)
            total = o if total is None else total + o
        outs[i][...] = jnp.concatenate([total[0:w], total[w:]], axis=1).astype(BF16)


def pack_rows(stage, rows, slot, first):
    count = rows.shape[0]
    for s in range(8):
        for k in range(2):
            at = s * 256 + k * 128
            stage[2 * slot + k, pl.ds(first + s, count, stride=8), :] = rows[:, at : at + 128]


def unpack_rows(stage, slot, first, out_ref, at, count):
    for s in range(8):
        for k in range(2):
            got = stage[2 * slot + k, pl.ds(first + s, count, stride=8), :]
            lane = s * 256 + k * 128
            out_ref[pl.ds(at, count), lane : lane + 128] = got.astype(BF16)


def load_stage(stage, ref, n):
    for k in range(2 * n):
        stage[k, 0 : ref.shape[0], :] = ref[:, k * 128 : (k + 1) * 128].astype(F32)


def store_stage(out_ref, stage, n):
    for k in range(2 * n):
        out_ref[:, k * 128 : (k + 1) * 128] = stage[k].astype(BF16)


def project_body(cap, half_ref, *refs):
    mine, theirs, (h1_ref, h2_ref, h3_ref), refs = refs[:6], refs[6:12], refs[12:15], refs[15:]
    h0_hbm, own_hbm, stream_hbm, gain_hbm, pick_hbm, mixed_hbm = refs[:6]
    outs, (stage, h0_ref, own_ref, stream_ref, gain_ref, pick_ref, mixed_ref, sems) = refs[6:-8], refs[-8:]
    fetched = fetch_all(
        (
            (h0_hbm, h0_ref),
            (own_hbm, own_ref),
            (stream_hbm, stream_ref),
            (gain_hbm, gain_ref),
            (pick_hbm, pick_ref),
        ),
        sems,
    )
    h1, h2, h3 = h1_ref[...], h2_ref[...], h3_ref[...]
    mid = mine[0].shape[0]
    wide = own_ref.shape[1] // 2
    sides = [x for h in (h1, h3, h2) for x in (h[:, :mid], h[:, mid:])]
    for half, parts in ((half_ref[0], mine), (1 - half_ref[0], theirs)):
        here = pl.ds(pl.multiple_of(half * wide, wide), wide)
        part = None
        for side, w in zip(sides, parts):
            one = dot(side, w[...])
            part = one if part is None else part + one
        mixed_ref[:, here] = part
    wait_all(fetched)
    mixed = mixed_ref[...] + dot(h0_ref[...], own_ref[...]) + stream_ref[...].astype(F32)
    mixed_ref[...] = mixed
    kept = pltpu.make_async_copy(mixed_ref, mixed_hbm, sems.at[5])
    kept.start()
    scale = lax.rsqrt(jnp.mean(mixed * mixed, axis=1, keepdims=True) + EPSILON)
    normed = (mixed * scale * gain_ref[...]).astype(BF16)
    experts = pick_ref.shape[0] // cap
    slot = 0
    for c, n in enumerate(CHUNKS):
        for r in range(n):
            rows = dot(pick_ref[slot * experts : (slot + 1) * experts, :], normed)
            pack_rows(stage, rows, r, 0)
            slot += 1
        store_stage(outs[c], stage, n)
    kept.wait()


def expert_body(n, ins, *refs):
    blocks, (gate_ref, up_ref, down_ref) = refs[:ins], refs[ins : ins + 3]
    outs, (stage, x, act, gates, ups, downs, sems) = refs[ins + 3 : -7], refs[-7:]
    h = outs[0].shape[0]
    srcs = h // n
    cols = act.shape[2]

    def fetch(i):
        here = pl.ds(pl.multiple_of(i * cols, cols), cols)
        return (
            pltpu.make_async_copy(gate_ref.at[0, :, here], gates.at[i], sems.at[0, i]),
            pltpu.make_async_copy(up_ref.at[0, :, here], ups.at[i], sems.at[1, i]),
        )

    def fetch_down():
        return pltpu.make_async_copy(down_ref.at[0], downs, sems.at[2, 0])

    for i in range(act.shape[0]):
        for copy in fetch(i):
            copy.start()
    fetch_down().start()
    row = 0
    for ref in blocks:
        load_stage(stage, ref, n)
        for half in range(ref.shape[0] // (8 * srcs)):
            first = row

            def one_slot(r, carry):
                unpack_rows(stage, r, half * 8 * srcs, x, pl.multiple_of(first + r * srcs, srcs), srcs)
                return carry

            lax.fori_loop(0, n, one_slot, 0)
            row += h

    def hidden_tile(i, carry):
        for copy in fetch(i):
            copy.wait()
        both = jnp.concatenate([gates[i], ups[i]], axis=1)
        gu = dot(x[...], both)
        g, u = gu[:, :cols], gu[:, cols:]
        act[i] = (g * (1.0 / (1.0 + jnp.exp(-g))) * u).astype(BF16)
        return carry

    lax.fori_loop(0, act.shape[0], hidden_tile, 0)
    fetch_down().wait()
    hid = jnp.concatenate([act[i] for i in range(act.shape[0])], axis=1)
    wide = 256

    def out_tile(t, carry):
        here = pl.ds(pl.multiple_of(t * wide, wide), wide)
        y = dot(hid, downs[:, here]).astype(BF16)
        for k, out in enumerate(outs):
            out[:, here] = y[k * h : (k + 1) * h]
        return carry

    lax.fori_loop(0, downs.shape[1] // wide, out_tile, 0)


def gathered_body(n, own_top, own_bottom, plus_ref, minus_ref, fromleft_ref, fromright_ref, out_ref, stage):
    h = fromleft_ref.shape[0]
    srcs = h // n
    top = own_top[...].astype(F32) + minus_ref[...].astype(F32) + fromleft_ref[...].astype(F32)
    bottom = own_bottom[...].astype(F32) + plus_ref[...].astype(F32) + fromright_ref[...].astype(F32)
    for half, rows in enumerate((top, bottom)):
        for r in range(n):
            pack_rows(stage, rows[r * srcs : (r + 1) * srcs], r, half * 8 * srcs)
    store_stage(out_ref, stage, n)


def combine_body(cap, *refs):
    rets, refs = refs[: len(CHUNKS)], refs[len(CHUNKS) :]
    pick0_hbm, pick1_hbm, wcol_hbm, mixed_hbm, out_ref, stage, back = refs[:7]
    pick0_ref, pick1_ref, wcol_ref, mixed_ref, sems = refs[7:]
    fetched = fetch_all(
        ((pick0_hbm, pick0_ref), (pick1_hbm, pick1_ref), (wcol_hbm, wcol_ref), (mixed_hbm, mixed_ref)), sems
    )
    experts = pick0_ref.shape[0] // cap
    slot = 0
    for ref, n in zip(rets, CHUNKS):
        load_stage(stage, ref, n)
        for r in range(n):
            unpack_rows(stage, r, 0, back, slot * experts, experts)
            slot += 1
    wait_all(fetched)
    rows = mixed_ref.shape[0]
    one = (((0,), (0,)), ((), ()))
    for t in range(mixed_ref.shape[1] // 256):
        here = slice(t * 256, (t + 1) * 256)
        o0 = lax.dot_general(pick0_ref[...], back[:, here], one, preferred_element_type=F32)
        o1 = lax.dot_general(pick1_ref[...], back[:, here], one, preferred_element_type=F32)
        for lane in range(0, 256, rows):
            at = slice(t * 256 + lane, t * 256 + lane + rows)
            out_ref[:, at] = (
                mixed_ref[:, at]
                + wcol_ref[:, :rows] * o0[:, lane : lane + rows]
                + wcol_ref[:, rows:] * o1[:, lane : lane + rows]
            ).astype(BF16)


def hop(even, odd):
    even = exchange(even, EVEN)
    odd = exchange(odd, ODD)
    return even, odd


def on_device(queries, keys, values, sink_logits, stream, out_proj, norm_gain, routes, route_weights,
              gate_proj, up_proj, down_proj):
    vmem = pl.BlockSpec(memory_space=pltpu.VMEM)
    smem = pl.BlockSpec(memory_space=pltpu.SMEM)
    hbm = pl.BlockSpec(memory_space=pltpu.HBM)
    tok_sp, width = queries.shape
    rows, d = stream.shape
    experts = lax.axis_size("sp")
    cap = max(2, (5 * rows + 2 * experts - 1) // (2 * experts))
    sp, tp = lax.axis_index("sp"), lax.axis_index("tp")
    key_t, value_t = keys.T, values.T

    core = lax.rem(sp, 2)
    mid, wide = width // 2, d // 2
    w_top, w_bottom, tail = call(
        split_body,
        [jax.ShapeDtypeStruct((mid, wide), BF16)] * 2 + [jax.ShapeDtypeStruct((2 * DH, WINDOW), BF16)],
        [pltpu.SemaphoreType.DMA((4,))],
        in_specs=[smem] + [hbm] * 3,
        out_specs=[vmem] * 3,
        mib=58,
    )(core.reshape(1), out_proj, key_t, value_t)
    tail = lax.ppermute(tail, "sp", [(i, i + 1) for i in range(experts - 1)])

    even_top, odd_bottom = hop(w_top, w_bottom)
    even_bottom, odd_top = hop(w_bottom, w_top)
    far_bottom, far_top = hop(odd_bottom, even_top)
    gathered_w = [even_top, even_bottom, odd_top, odd_bottom, far_top, far_bottom]
    for k in range(6):
        gathered_w.append(partner(gathered_w[k]))

    slots = experts * cap
    pick, pick0, pick1, wcol = call(
        functools.partial(route_body, cap),
        [jax.ShapeDtypeStruct((slots, rows), BF16)] * 3 + [jax.ShapeDtypeStruct((rows, 2 * rows), F32)],
        [pltpu.VMEM((2, rows), jnp.int32), pltpu.VMEM((2, rows), F32), pltpu.SemaphoreType.DMA((2,))],
        in_specs=[hbm] * 2,
        out_specs=[vmem] * 4,
        mib=8,
    )(routes.T, route_weights.T)

    heads = call(
        attend_body,
        [jax.ShapeDtypeStruct((WINDOW, width), BF16)] * 4,
        [pltpu.VMEM((DH, tok_sp + WINDOW), BF16)] * 2
        + [
            pltpu.VMEM((tok_sp, width), BF16),
            pltpu.VMEM((DH, tok_sp), BF16),
            pltpu.VMEM((DH, tok_sp), BF16),
            pltpu.SemaphoreType.DMA((3,)),
        ],
        in_specs=[smem, smem, smem, hbm, hbm, hbm, vmem],
        out_specs=[vmem] * 4,
        mib=58,
    )(tp.reshape(1), (sp == 0).astype(jnp.int32).reshape(1), sink_logits, queries, key_t, value_t, tail)
    heads = list(heads)
    for i in (1, 2, 3):
        heads[i] = exchange(heads[i], (EVEN, ACROSS, ODD)[i - 1])

    mixed, *outgoing = call(
        functools.partial(project_body, cap),
        [jax.ShapeDtypeStruct((rows, d), F32)]
        + [jax.ShapeDtypeStruct((experts * 8, 256 * n), BF16) for n in CHUNKS],
        [
            pltpu.VMEM((2 * max(CHUNKS), experts * 8, 128), F32),
            pltpu.VMEM((WINDOW, width), BF16),
            pltpu.VMEM((width, d), BF16),
            pltpu.VMEM((rows, d), BF16),
            pltpu.VMEM((1, d), F32),
            pltpu.VMEM((slots, rows), BF16),
            pltpu.VMEM((rows, d), F32),
            pltpu.SemaphoreType.DMA((6,)),
        ],
        in_specs=[smem] + [vmem] * 15 + [hbm] * 5,
        out_specs=[hbm] + [vmem] * len(CHUNKS),
        mib=20,
    )(core.reshape(1), *gathered_w, *heads[1:], heads[0], out_proj, stream,
      norm_gain.reshape(1, d), pick)

    vm = lambda k: [vmem] * k
    cols = 128
    hidden = gate_proj.shape[2]
    n = CHUNKS[0]
    h = experts * n // 2
    add = lambda a, b: (a.astype(F32) + b.astype(F32)).astype(BF16)
    tie = lax.optimization_barrier

    def run_experts(*blocks):
        tall = sum(v.shape[0] for v in blocks) // 8 * n
        return call(
            functools.partial(expert_body, n, len(blocks)),
            [jax.ShapeDtypeStruct((h, d), BF16)] * (tall // h),
            [
                pltpu.VMEM((2 * n, experts * 8, 128), F32),
                pltpu.VMEM((tall, d), BF16),
                pltpu.VMEM((hidden // cols, tall, cols), BF16),
                pltpu.VMEM((hidden // cols, d, cols), BF16),
                pltpu.VMEM((hidden // cols, d, cols), BF16),
                pltpu.VMEM((hidden, d), BF16),
                pltpu.SemaphoreType.DMA((3, hidden // cols)),
            ],
            in_specs=vm(len(blocks)) + [hbm] * 3,
            out_specs=vm(tall // h),
            mib=28,
            cost_estimate=pl.CostEstimate(
                flops=6 * tall * d * hidden, transcendentals=tall * hidden, bytes_accessed=6 * d * hidden
            ),
        )(*blocks, gate_proj, up_proj, down_proj)

    block = outgoing[0].reshape(experts, 8, 256 * n)
    arrived = lax.all_to_all(block, "sp", 0, 0, tiled=True).reshape(experts * 8, 256 * n)
    half = experts * 4
    top, bottom = arrived[:half], arrived[half:]
    even_top, odd_bottom = hop(top, bottom)
    even_bottom, odd_top = hop(bottom, top)
    own_top, own_bottom = run_experts(arrived)
    even_top, odd_bottom, own_top = tie((even_top, odd_bottom, own_top))
    far_bottom, far_top = hop(odd_bottom, even_top)
    e_top, e_bottom, o_top, o_bottom = run_experts(even_top, even_bottom, odd_top, odd_bottom)
    plus, minus = hop(e_bottom, o_top)
    y_top, y_bottom = run_experts(far_top, far_bottom)
    y_bottom, y_top = hop(y_bottom, y_top)
    from_even, from_odd = hop(add(e_top, y_top), add(o_bottom, y_bottom))
    back = call(
        functools.partial(gathered_body, n),
        jax.ShapeDtypeStruct((experts * 8, 256 * n), BF16),
        [pltpu.VMEM((2 * n, experts * 8, 128), F32)],
        in_specs=vm(6),
        out_specs=vmem,
    )(own_top, own_bottom, plus, minus, from_even, from_odd)
    back = lax.all_to_all(back.reshape(experts, 8, 256 * n), "sp", 0, 0, tiled=True)
    returned = [back.reshape(experts * 8, 256 * n)]

    return call(
        functools.partial(combine_body, cap),
        jax.ShapeDtypeStruct((rows, d), BF16),
        [
            pltpu.VMEM((2 * max(CHUNKS), experts * 8, 128), F32),
            pltpu.VMEM((slots, d), BF16),
            pltpu.VMEM((slots, rows), BF16),
            pltpu.VMEM((slots, rows), BF16),
            pltpu.VMEM((rows, 2 * rows), F32),
            pltpu.VMEM((rows, d), F32),
            pltpu.SemaphoreType.DMA((4,)),
        ],
        in_specs=vm(len(CHUNKS)) + [hbm] * 4,
        out_specs=vmem,
        mib=20,
    )(*returned, pick0, pick1, wcol, mixed)


def solution(mesh):
    return jax.shard_map(
        on_device,
        mesh=mesh,
        in_specs=(
            P("sp", "tp"),
            P("sp", "tp"),
            P("sp", "tp"),
            P("tp"),
            P(("sp", "tp"), None),
            P("tp", None),
            P(),
            P(("sp", "tp"), None),
            P(("sp", "tp"), None),
            P("sp", None, "tp"),
            P("sp", None, "tp"),
            P("sp", "tp", None),
        ),
        out_specs=P(("sp", "tp"), None),
        check_vma=False,
    )
```

```python
import functools
import jax
import jax.numpy as jnp
from jax import lax
from jax.experimental import pallas as pl
from jax.experimental.pallas import tpu as pltpu
from jax.sharding import PartitionSpec as P


DH = 64
WINDOW = 128
EPSILON = 1e-06
CHUNKS = (5,)

F32 = jnp.float32
BF16 = jnp.bfloat16


EVEN, ACROSS, ODD = (1, 0, 3, 2), (2, 3, 0, 1), (3, 2, 1, 0)


def exchange(value, peers):
    return lax.ppermute(value, "tp", list(enumerate(peers)))


def partner(value):
    n = lax.axis_size("sp")
    return lax.ppermute(value, "sp", [(i, i ^ 1) for i in range(n)])


def dot(a, b):
    return jnp.dot(a, b, preferred_element_type=F32)


def call(body, outs, scratch=(), mib=16, **kw):
    return pl.pallas_call(
        body,
        out_shape=outs,
        scratch_shapes=list(scratch),
        compiler_params=pltpu.CompilerParams(vmem_limit_bytes=mib << 20),
        **kw,
    )


def fetch_all(pairs, sems):
    copies = [pltpu.make_async_copy(src, dst, sems.at[i]) for i, (src, dst) in enumerate(pairs)]
    for copy in copies:
        copy.start()
    return copies


def wait_all(copies):
    for copy in copies:
        copy.wait()


def route_body(cap, routes_hbm, w_hbm, pick_ref, across_ref, wcol_ref, routes_ref, w_ref, sems):
    wait_all(fetch_all(((routes_hbm, routes_ref), (w_hbm, w_ref)), sems))
    rows = routes_ref.shape[1]
    experts = pick_ref.shape[0] // cap
    ids = lax.broadcasted_iota(jnp.int32, (experts, rows), 0)
    before = (
        lax.broadcasted_iota(jnp.int32, (rows, rows), 0)
        < lax.broadcasted_iota(jnp.int32, (rows, rows), 1)
    ).astype(F32).astype(BF16)
    hit0 = (ids == routes_ref[0:1, :]).astype(F32)
    hit1 = (ids == routes_ref[1:2, :]).astype(F32)
    rank0 = dot(hit0.astype(BF16), before)
    rank1 = dot(hit1.astype(BF16), before) + jnp.sum(hit0, axis=1, keepdims=True)
    firsts, seconds = [], []
    for r in range(cap):
        at0 = jnp.where(rank0 == float(r), hit0, 0.0)
        at1 = jnp.where(rank1 == float(r), hit1, 0.0)
        here = slice(r * experts, (r + 1) * experts)
        firsts.append(at0)
        seconds.append(at1)
        pick_ref[here, :] = (at0 + at1).astype(BF16)
    for k, parts in enumerate((firsts, seconds)):
        across_ref[k * rows : (k + 1) * rows, :] = jnp.concatenate(parts, axis=0).T.astype(BF16)
        spread = jnp.broadcast_to(w_ref[k : k + 1, :], (rows, rows))
        wcol_ref[:, k * rows : (k + 1) * rows] = spread.T


def split_body(half_ref, w_hbm, k_hbm, v_hbm, top_ref, bottom_ref, tail_ref, sems):
    mid, wide = top_ref.shape
    cols = pl.ds(pl.multiple_of(half_ref[0] * wide, wide), wide)
    last = pl.ds(k_hbm.shape[1] - WINDOW, WINDOW)
    copies = fetch_all(
        (
            (w_hbm.at[0:mid, cols], top_ref),
            (w_hbm.at[mid : 2 * mid, cols], bottom_ref),
            (k_hbm.at[:, last], tail_ref.at[0:DH, :]),
            (v_hbm.at[:, last], tail_ref.at[DH : 2 * DH, :]),
        ),
        sems,
    )
    wait_all(copies)


def attend_body(me_ref, first_ref, sink_ref, q_hbm, k_hbm, v_hbm, tail_ref, *refs):
    outs, (band_k, band_v, q_ref, k_ref, v_ref, sems) = refs[:4], refs[4:]
    copies = fetch_all(((q_hbm, q_ref), (k_hbm, k_ref), (v_hbm, v_ref)), sems)
    w = WINDOW
    band_k[0:DH, 0:w] = tail_ref[0:DH, :]
    band_v[0:DH, 0:w] = tail_ref[DH : 2 * DH, :]
    wait_all(copies)
    band_k[0:DH, w:] = k_ref[...]
    band_v[0:DH, w:] = v_ref[...]
    qpos = lax.broadcasted_iota(jnp.int32, (2 * w, 2 * w), 0) % w
    kpos = lax.broadcasted_iota(jnp.int32, (2 * w, 2 * w), 1)
    near = (kpos > qpos) & (kpos <= qpos + w)
    lower = lax.broadcasted_iota(jnp.int32, (2 * w, 1), 0) < w
    zero = jnp.zeros((DH, 2 * w), BF16)
    for i in range(4):
        n = me_ref[0] ^ i
        at = pl.multiple_of(n * w, w)
        kb = band_k[0:DH, pl.ds(at, 2 * w)]
        vb = band_v[0:DH, pl.ds(at, 2 * w)]
        hidden = jnp.where((first_ref[0] == 1) & (n == 0), w, 0)
        allowed = near & (kpos >= hidden)
        qb = q_ref[pl.ds(at, w), :]
        q2 = jnp.concatenate([qb[:, 0:w], qb[:, w:]], axis=0)
        total = None
        for h in range(2):
            kz = jnp.concatenate([kb, zero] if h == 0 else [zero, kb], axis=0)
            vz = jnp.concatenate([vb, zero] if h == 0 else [zero, vb], axis=0)
            s = dot(q2, kz) * DH ** (-0.5)
            s = jnp.where(allowed, s, -jnp.inf)
            sink = jnp.where(lower, sink_ref[h], sink_ref[2 + h])
            top = jnp.maximum(jnp.max(s, axis=1, keepdims=True), sink)
            e = jnp.exp(s - top)
            den = jnp.sum(e, axis=1, keepdims=True) + jnp.exp(sink - top)
            p = (e / den).astype(BF16)
            o = lax.dot_general(p, vz, (((1,), (1,)), ((), ())), preferred_element_type=F32)
            total = o if total is None else total + o
        outs[i][...] = jnp.concatenate([total[0:w], total[w:]], axis=1).astype(BF16)


def pack_rows(stage, rows, slot, first):
    count = rows.shape[0]
    for s in range(8):
        for k in range(2):
            at = s * 256 + k * 128
            stage[2 * slot + k, pl.ds(first + s, count, stride=8), :] = rows[:, at : at + 128]


def unpack_rows(stage, slot, first, out_ref, at, count):
    for s in range(8):
        for k in range(2):
            got = stage[2 * slot + k, pl.ds(first + s, count, stride=8), :]
            lane = s * 256 + k * 128
            out_ref[pl.ds(at, count), lane : lane + 128] = got.astype(BF16)


def load_stage(stage, ref, n):
    for k in range(2 * n):
        stage[k, 0 : ref.shape[0], :] = ref[:, k * 128 : (k + 1) * 128].astype(F32)


def store_stage(out_ref, stage, n):
    for k in range(2 * n):
        out_ref[:, k * 128 : (k + 1) * 128] = stage[k].astype(BF16)


def project_body(cap, half_ref, *refs):
    mine, theirs, (h1_ref, h2_ref, h3_ref), refs = refs[:6], refs[6:12], refs[12:15], refs[15:]
    h0_hbm, own_hbm, stream_hbm, gain_hbm, pick_hbm, mixed_hbm = refs[:6]
    outs, (stage, h0_ref, own_ref, stream_ref, gain_ref, pick_ref, mixed_ref, sems) = refs[6:-8], refs[-8:]
    fetched = fetch_all(
        (
            (h0_hbm, h0_ref),
            (own_hbm, own_ref),
            (stream_hbm, stream_ref),
            (gain_hbm, gain_ref),
            (pick_hbm, pick_ref),
        ),
        sems,
    )
    h1, h2, h3 = h1_ref[...], h2_ref[...], h3_ref[...]
    mid = mine[0].shape[0]
    wide = own_ref.shape[1] // 2
    sides = [x for h in (h1, h3, h2) for x in (h[:, :mid], h[:, mid:])]
    for half, parts in ((half_ref[0], mine), (1 - half_ref[0], theirs)):
        here = pl.ds(pl.multiple_of(half * wide, wide), wide)
        part = None
        for side, w in zip(sides, parts):
            one = dot(side, w[...])
            part = one if part is None else part + one
        mixed_ref[:, here] = part
    wait_all(fetched)
    mixed = mixed_ref[...] + dot(h0_ref[...], own_ref[...]) + stream_ref[...].astype(F32)
    mixed_ref[...] = mixed
    kept = pltpu.make_async_copy(mixed_ref, mixed_hbm, sems.at[5])
    kept.start()
    scale = lax.rsqrt(jnp.mean(mixed * mixed, axis=1, keepdims=True) + EPSILON)
    normed = (mixed * scale * gain_ref[...]).astype(BF16)
    experts = pick_ref.shape[0] // cap
    slot = 0
    for c, n in enumerate(CHUNKS):
        for r in range(n):
            rows = dot(pick_ref[slot * experts : (slot + 1) * experts, :], normed)
            pack_rows(stage, rows, r, 0)
            slot += 1
        store_stage(outs[c], stage, n)
    kept.wait()


def expert_body(n, ins, *refs):
    blocks, (gate_ref, up_ref, down_ref) = refs[:ins], refs[ins : ins + 3]
    outs, (stage, x, act, gates, ups, downs, sems) = refs[ins + 3 : -7], refs[-7:]
    h = outs[0].shape[0]
    srcs = h // n
    cols = act.shape[2]

    def fetch(i):
        here = pl.ds(pl.multiple_of(i * cols, cols), cols)
        return (
            pltpu.make_async_copy(gate_ref.at[0, :, here], gates.at[i], sems.at[0, i]),
            pltpu.make_async_copy(up_ref.at[0, :, here], ups.at[i], sems.at[1, i]),
        )

    def fetch_down():
        return pltpu.make_async_copy(down_ref.at[0], downs, sems.at[2, 0])

    for i in range(act.shape[0]):
        for copy in fetch(i):
            copy.start()
    fetch_down().start()
    row = 0
    for ref in blocks:
        load_stage(stage, ref, n)
        for half in range(ref.shape[0] // (8 * srcs)):
            first = row

            def one_slot(r, carry):
                unpack_rows(stage, r, half * 8 * srcs, x, pl.multiple_of(first + r * srcs, srcs), srcs)
                return carry

            lax.fori_loop(0, n, one_slot, 0)
            row += h

    def hidden_tile(i, carry):
        for copy in fetch(i):
            copy.wait()
        both = jnp.concatenate([gates[i], ups[i]], axis=1)
        gu = dot(x[...], both)
        g, u = gu[:, :cols], gu[:, cols:]
        act[i] = (g * (1.0 / (1.0 + jnp.exp(-g))) * u).astype(BF16)
        return carry

    lax.fori_loop(0, act.shape[0], hidden_tile, 0)
    fetch_down().wait()
    hid = jnp.concatenate([act[i] for i in range(act.shape[0])], axis=1)
    wide = 256

    def out_tile(t, carry):
        here = pl.ds(pl.multiple_of(t * wide, wide), wide)
        y = dot(hid, downs[:, here]).astype(BF16)
        for k, out in enumerate(outs):
            out[:, here] = y[k * h : (k + 1) * h]
        return carry

    lax.fori_loop(0, downs.shape[1] // wide, out_tile, 0)


def gathered_body(n, own_top, own_bottom, plus_ref, minus_ref, fromleft_ref, fromright_ref, out_ref, stage):
    h = fromleft_ref.shape[0]
    srcs = h // n
    top = own_top[...].astype(F32) + minus_ref[...].astype(F32) + fromleft_ref[...].astype(F32)
    bottom = own_bottom[...].astype(F32) + plus_ref[...].astype(F32) + fromright_ref[...].astype(F32)
    for half, rows in enumerate((top, bottom)):
        for r in range(n):
            pack_rows(stage, rows[r * srcs : (r + 1) * srcs], r, half * 8 * srcs)
    store_stage(out_ref, stage, n)


def combine_body(cap, *refs):
    rets, refs = refs[: len(CHUNKS)], refs[len(CHUNKS) :]
    across_hbm, wcol_hbm, mixed_hbm, out_ref, stage, back = refs[:6]
    across_ref, wcol_ref, mixed_ref, sems = refs[6:]
    fetched = fetch_all(((across_hbm, across_ref), (wcol_hbm, wcol_ref), (mixed_hbm, mixed_ref)), sems)
    experts = across_ref.shape[1] // cap
    slot = 0
    for ref, n in zip(rets, CHUNKS):
        load_stage(stage, ref, n)
        for r in range(n):
            unpack_rows(stage, r, 0, back, slot * experts, experts)
            slot += 1
    wait_all(fetched)
    rows = mixed_ref.shape[0]
    for t in range(mixed_ref.shape[1] // 256):
        both = dot(across_ref[...], back[:, t * 256 : (t + 1) * 256])
        o0, o1 = both[:rows], both[rows:]
        for lane in range(0, 256, rows):
            at = slice(t * 256 + lane, t * 256 + lane + rows)
            out_ref[:, at] = (
                mixed_ref[:, at]
                + wcol_ref[:, :rows] * o0[:, lane : lane + rows]
                + wcol_ref[:, rows:] * o1[:, lane : lane + rows]
            ).astype(BF16)


def hop(even, odd):
    even = exchange(even, EVEN)
    odd = exchange(odd, ODD)
    return even, odd


def on_device(queries, keys, values, sink_logits, stream, out_proj, norm_gain, routes, route_weights,
              gate_proj, up_proj, down_proj):
    vmem = pl.BlockSpec(memory_space=pltpu.VMEM)
    smem = pl.BlockSpec(memory_space=pltpu.SMEM)
    hbm = pl.BlockSpec(memory_space=pltpu.HBM)
    tok_sp, width = queries.shape
    rows, d = stream.shape
    experts = lax.axis_size("sp")
    cap = max(2, (5 * rows + 2 * experts - 1) // (2 * experts))
    sp, tp = lax.axis_index("sp"), lax.axis_index("tp")
    key_t, value_t = keys.T, values.T

    core = lax.rem(sp, 2)
    mid, wide = width // 2, d // 2
    w_top, w_bottom, tail = call(
        split_body,
        [jax.ShapeDtypeStruct((mid, wide), BF16)] * 2 + [jax.ShapeDtypeStruct((2 * DH, WINDOW), BF16)],
        [pltpu.SemaphoreType.DMA((4,))],
        in_specs=[smem] + [hbm] * 3,
        out_specs=[vmem] * 3,
        mib=58,
    )(core.reshape(1), out_proj, key_t, value_t)
    tail = lax.ppermute(tail, "sp", [(i, i + 1) for i in range(experts - 1)])

    even_top, odd_bottom = hop(w_top, w_bottom)
    even_bottom, odd_top = hop(w_bottom, w_top)
    far_bottom, far_top = hop(odd_bottom, even_top)
    gathered_w = [even_top, even_bottom, odd_top, odd_bottom, far_top, far_bottom]
    for k in range(6):
        gathered_w.append(partner(gathered_w[k]))

    slots = experts * cap
    pick, across, wcol = call(
        functools.partial(route_body, cap),
        [jax.ShapeDtypeStruct((slots, rows), BF16), jax.ShapeDtypeStruct((2 * rows, slots), BF16)] + [jax.ShapeDtypeStruct((rows, 2 * rows), F32)],
        [pltpu.VMEM((2, rows), jnp.int32), pltpu.VMEM((2, rows), F32), pltpu.SemaphoreType.DMA((2,))],
        in_specs=[hbm] * 2,
        out_specs=[vmem] * 3,
        mib=8,
    )(routes.T, route_weights.T)

    heads = call(
        attend_body,
        [jax.ShapeDtypeStruct((WINDOW, width), BF16)] * 4,
        [pltpu.VMEM((DH, tok_sp + WINDOW), BF16)] * 2
        + [
            pltpu.VMEM((tok_sp, width), BF16),
            pltpu.VMEM((DH, tok_sp), BF16),
            pltpu.VMEM((DH, tok_sp), BF16),
            pltpu.SemaphoreType.DMA((3,)),
        ],
        in_specs=[smem, smem, smem, hbm, hbm, hbm, vmem],
        out_specs=[vmem] * 4,
        mib=58,
    )(tp.reshape(1), (sp == 0).astype(jnp.int32).reshape(1), sink_logits, queries, key_t, value_t, tail)
    heads = list(heads)
    for i in (1, 2, 3):
        heads[i] = exchange(heads[i], (EVEN, ACROSS, ODD)[i - 1])

    mixed, *outgoing = call(
        functools.partial(project_body, cap),
        [jax.ShapeDtypeStruct((rows, d), F32)]
        + [jax.ShapeDtypeStruct((experts * 8, 256 * n), BF16) for n in CHUNKS],
        [
            pltpu.VMEM((2 * max(CHUNKS), experts * 8, 128), F32),
            pltpu.VMEM((WINDOW, width), BF16),
            pltpu.VMEM((width, d), BF16),
            pltpu.VMEM((rows, d), BF16),
            pltpu.VMEM((1, d), F32),
            pltpu.VMEM((slots, rows), BF16),
            pltpu.VMEM((rows, d), F32),
            pltpu.SemaphoreType.DMA((6,)),
        ],
        in_specs=[smem] + [vmem] * 15 + [hbm] * 5,
        out_specs=[hbm] + [vmem] * len(CHUNKS),
        mib=20,
    )(core.reshape(1), *gathered_w, *heads[1:], heads[0], out_proj, stream,
      norm_gain.reshape(1, d), pick)

    vm = lambda k: [vmem] * k
    cols = 128
    hidden = gate_proj.shape[2]
    n = CHUNKS[0]
    h = experts * n // 2
    add = lambda a, b: (a.astype(F32) + b.astype(F32)).astype(BF16)
    tie = lax.optimization_barrier

    def run_experts(*blocks):
        tall = sum(v.shape[0] for v in blocks) // 8 * n
        return call(
            functools.partial(expert_body, n, len(blocks)),
            [jax.ShapeDtypeStruct((h, d), BF16)] * (tall // h),
            [
                pltpu.VMEM((2 * n, experts * 8, 128), F32),
                pltpu.VMEM((tall, d), BF16),
                pltpu.VMEM((hidden // cols, tall, cols), BF16),
                pltpu.VMEM((hidden // cols, d, cols), BF16),
                pltpu.VMEM((hidden // cols, d, cols), BF16),
                pltpu.VMEM((hidden, d), BF16),
                pltpu.SemaphoreType.DMA((3, hidden // cols)),
            ],
            in_specs=vm(len(blocks)) + [hbm] * 3,
            out_specs=vm(tall // h),
            mib=28,
            cost_estimate=pl.CostEstimate(
                flops=6 * tall * d * hidden, transcendentals=tall * hidden, bytes_accessed=6 * d * hidden
            ),
        )(*blocks, gate_proj, up_proj, down_proj)

    block = outgoing[0].reshape(experts, 8, 256 * n)
    arrived = lax.all_to_all(block, "sp", 0, 0, tiled=True).reshape(experts * 8, 256 * n)
    half = experts * 4
    top, bottom = arrived[:half], arrived[half:]
    even_top, odd_bottom = hop(top, bottom)
    even_bottom, odd_top = hop(bottom, top)
    own_top, own_bottom = run_experts(arrived)
    even_top, odd_bottom, own_top = tie((even_top, odd_bottom, own_top))
    far_bottom, far_top = hop(odd_bottom, even_top)
    e_top, e_bottom, o_top, o_bottom = run_experts(even_top, even_bottom, odd_top, odd_bottom)
    plus, minus = hop(e_bottom, o_top)
    y_top, y_bottom = run_experts(far_top, far_bottom)
    y_bottom, y_top = hop(y_bottom, y_top)
    from_even, from_odd = hop(add(e_top, y_top), add(o_bottom, y_bottom))
    back = call(
        functools.partial(gathered_body, n),
        jax.ShapeDtypeStruct((experts * 8, 256 * n), BF16),
        [pltpu.VMEM((2 * n, experts * 8, 128), F32)],
        in_specs=vm(6),
        out_specs=vmem,
    )(own_top, own_bottom, plus, minus, from_even, from_odd)
    back = lax.all_to_all(back.reshape(experts, 8, 256 * n), "sp", 0, 0, tiled=True)
    returned = [back.reshape(experts * 8, 256 * n)]

    return call(
        functools.partial(combine_body, cap),
        jax.ShapeDtypeStruct((rows, d), BF16),
        [
            pltpu.VMEM((2 * max(CHUNKS), experts * 8, 128), F32),
            pltpu.VMEM((slots, d), BF16),
            pltpu.VMEM((2 * rows, slots), BF16),
            pltpu.VMEM((rows, 2 * rows), F32),
            pltpu.VMEM((rows, d), F32),
            pltpu.SemaphoreType.DMA((3,)),
        ],
        in_specs=vm(len(CHUNKS)) + [hbm] * 3,
        out_specs=vmem,
        mib=20,
    )(*returned, across, wcol, mixed)


def solution(mesh):
    return jax.shard_map(
        on_device,
        mesh=mesh,
        in_specs=(
            P("sp", "tp"),
            P("sp", "tp"),
            P("sp", "tp"),
            P("tp"),
            P(("sp", "tp"), None),
            P("tp", None),
            P(),
            P(("sp", "tp"), None),
            P(("sp", "tp"), None),
            P("sp", None, "tp"),
            P("sp", None, "tp"),
            P("sp", "tp", None),
        ),
        out_specs=P(("sp", "tp"), None),
        check_vma=False,
    )
```
